256 devices in a mesh: ep: 16 (over y, x), tp: 16 (over z, core).
Axes of the slice: x: 4, y: 4, z: 8, core: 2. Of those that a mesh axis runs over, the one named last changes fastest.
Arguments:
- tokens: bfloat16 [2048, 2048], P('ep'), may hold values from -6 to 6
- conv_state: bfloat16 [2048, 3, 2048], P('ep', None, 'tp'), may hold values from -6 to 6
- rec_state: float32 [2048, 2048], P('ep', 'tp'), may hold values from -6 to 6
- gate_proj: bfloat16 [2048, 2048], P(None, 'tp'), may hold values from -0.125 to 0.125
- input_proj: bfloat16 [2048, 2048], P(None, 'tp'), may hold values from -0.125 to 0.125
- conv_taps: bfloat16 [4, 2048], P(None, 'tp'), may hold values from -3 to 3
- decay_blocks: bfloat16 [16, 128, 128], P('tp'), may hold values from -0.5 to 0.5
- input_blocks: bfloat16 [16, 128, 128], P('tp'), may hold values from -0.5 to 0.5
- decay_param: float32 [2048], P('tp'), may hold values from 0 to 6
- out_proj: bfloat16 [2048, 2048], P('tp'), may hold values from -0.125 to 0.125
- first_gain: float32 [2048], replicated, may hold values from 0.1 to 1.9
- expert_gate: bfloat16 [16, 2048, 7168], P('ep', None, 'tp'), may hold values from -0.125 to 0.125
- expert_up: bfloat16 [16, 2048, 7168], P('ep', None, 'tp'), may hold values from -0.125 to 0.125
- expert_down: bfloat16 [16, 7168, 2048], P('ep', 'tp'), may hold values from -0.0625 to 0.0625
- routing: int32 [2048, 2], P('ep'), may hold values from 0 to 15, all different within a row; in each aligned block of 128 rows (0 to 127, 128 to 255, ...) at most 32 rows name the same one
- route_weight: float32 [2048, 2], P('ep'), may hold values from 0.1 to 1
- dense_gate: bfloat16 [2048, 2048], P(None, 'tp'), may hold values from -0.125 to 0.125
- dense_up: bfloat16 [2048, 2048], P(None, 'tp'), may hold values from -0.125 to 0.125
- dense_down: bfloat16 [2048, 2048], P('tp'), may hold values from -0.125 to 0.125
- mix_weight: bfloat16 [2048], replicated, may hold values from -0.125 to 0.125
- second_gain: float32 [2048], P('tp'), may hold values from 0.1 to 1.9
Outputs:
- layer_out: bfloat16 [2048, 2048], P('ep', 'tp')
- new_state: float32 [2048, 2048], P('ep', 'tp')
- new_conv: bfloat16 [2048, 3, 2048], P('ep', None, 'tp')
The draws below stay inside these ranges and needn't reach their ends.
Inputs may be any that keep to these rules, and one draw needn't show every extreme that they name: `routing`: each row names 2 different experts; in each aligned block of 128 rows (the rows of one index of ep) no expert is named by more than 32 rows, a bound that some expert reaches in some block.
All inputs are finite; a program needn't handle non-finite values.
Results may differ from the reference program's by a relative error of at most 0.013.
Values may be sent and summed in bfloat16 or wider, within the bound.
A program may use at most 64 MiB of HBM per device.

```python
import math
import jax
import jax.numpy as jnp
import numpy as np
from jax import lax

D = 2048
DR = 2048
HEADS = 16
BLK = 128
FF = 7168
DFF_D = 2048
TOPK = 2
SEQ_GRP = 128
EXPERTS = 16
CAP = 32
BATCH = 2048
N_EP = 16
N_TP = 16


def steps_of(stream_key, extent, cuts, smallest, high):
    factor_of = 1.0
    for axis_at, parts in cuts:
        draws = jax.random.uniform(jax.random.fold_in(jax.random.fold_in(stream_key, 6), axis_at), (parts,), jnp.float32, smallest / len(cuts), high / len(cuts))
        factor_of = factor_of * jnp.repeat(jnp.exp(draws), extent[axis_at] // parts).reshape((-1,) + (1,) * (len(extent) - 1 - axis_at))
    return factor_of


def assign_block(rng, own, number, rows, amount, top, bound, skew):
    sequence = jax.random.permutation(rng, amount)
    packed, usual = shares(amount, rows * top, bound, skew, True), shares(amount, rows * top, bound, skew, False)
    places = jnp.arange(amount)

    def named(sizes, offset_by):
        used = int((sizes > 0).sum())
        fixed = max(1, used // 4)
        passed = fixed + (places - fixed + offset_by * (used - fixed)) % max(1, amount - fixed)
        return jnp.zeros((amount,), jnp.int32).at[sequence[jnp.where(places < fixed, places, passed)]].set(jnp.asarray(sizes, jnp.int32))

    sizes = jnp.where(number % 4 == 0, named(packed, number // 4), named(usual, number - number // 4 - 1))
    mixed = jax.random.permutation(jax.random.fold_in(own, 3), amount)
    giver, taker = mixed[0:amount // 2 * 2:2], mixed[1:amount // 2 * 2:2]
    slack = jnp.minimum(sizes[giver] - 1, bound - sizes[taker]) // 2
    slack = jnp.where((giver == sequence[0]) | (taker == sequence[0]) | (sizes[taker] == 0), 0, jnp.maximum(slack, 0))
    passed = jax.random.randint(jax.random.fold_in(own, 4), (amount // 2,), 0, 1 << 20) % (slack + 1)
    sizes = sizes.at[giver].add(-passed).at[taker].add(passed)
    items = jnp.searchsorted(jnp.cumsum(sizes), jnp.arange(rows * top), side="right").astype(jnp.int32)
    listing = items.reshape(top, rows).T
    listing = listing[jax.random.permutation(jax.random.fold_in(own, 1), rows)]
    offset_by = jax.random.randint(jax.random.fold_in(own, 2), (rows, 1), 0, top)
    return jnp.take_along_axis(listing, (jnp.arange(top)[None, :] + offset_by) % top, axis=1)


def shares(amount, total, bound, lean, full):
    weights = [(1 << 20) // math.isqrt(rank ** lean) + 1 for rank in range(1, amount + 1)]
    largest = bound if full else min(bound, max(-(-total // amount), total * weights[0] // sum(weights)))
    least = 1 if total - largest >= amount - 1 else 0
    given, surplus = [largest] + [least] * (amount - 1), total - largest - least * (amount - 1)
    while surplus > 0:
        free = [i for i in range(1, amount) if given[i] < largest] or [i for i in range(1, amount) if given[i] < bound]
        mass, remaining = sum([weights[i] for i in free]), surplus
        for i in free:
            extra = min(bound - given[i], max(1, remaining * weights[i] // mass), surplus)
            given[i] = given[i] + extra
            surplus = surplus - extra
    return np.array(given)


def normal_values(rng, shape, width, bound, split=(), held_as=jnp.bfloat16):
    factor_of = steps_of(rng, shape, split, -0.22, 0.18) if split else 1.0
    array = jax.random.normal(rng, shape, jnp.float32) * width * factor_of
    return jnp.minimum(jnp.maximum(array, -bound), bound).astype(held_as)


def setup_inputs(seed: int = 0) -> dict:
    key_of = jax.random.split(jax.random.key(seed), 22)
    tokens = normal_values(key_of[0], (BATCH, D), 1.0, 6.0, ((0, 16),))
    conv_state = normal_values(key_of[1], (BATCH, 3, DR), 1.0, 6.0, ((0, 16), (2, 16)))
    rec_state = normal_values(key_of[2], (BATCH, DR), 1.0, 6.0, ((0, 16), (1, 16)), jnp.float32)
    gate_proj = normal_values(key_of[3], (D, DR), D ** -0.5, 0.125, ((1, 16),))
    input_proj = normal_values(key_of[4], (D, DR), D ** -0.5, 0.125, ((1, 16),))
    conv_taps = normal_values(key_of[5], (4, DR), 4 ** -0.5, 3.0, ((1, 16),))
    decay_blocks = normal_values(key_of[6], (HEADS, BLK, BLK), BLK ** -0.5, 0.5, ((0, 16),))
    input_blocks = normal_values(key_of[7], (HEADS, BLK, BLK), BLK ** -0.5, 0.5, ((0, 16),))
    decay_param = jnp.clip(6.0 * jax.random.uniform(key_of[8], (DR,), jnp.float32) ** steps_of(key_of[8], (DR,), ((0, 16),), -0.2, 0.2), 0.0, 6.0)
    out_proj = normal_values(key_of[9], (DR, D), DR ** -0.5, 0.125, ((0, 16),))
    first_gain = jnp.clip(1.0 + 0.18 * jax.random.normal(key_of[10], (D,), jnp.float32), 0.1, 1.9)
    expert_gate = normal_values(key_of[11], (EXPERTS, D, FF), D ** -0.5, 0.125, ((0, 16), (2, 16)))
    expert_up = normal_values(key_of[12], (EXPERTS, D, FF), D ** -0.5, 0.125, ((0, 16), (2, 16)))
    expert_down = normal_values(key_of[13], (EXPERTS, FF, D), FF ** -0.5, 0.0625, ((0, 16), (1, 16)))
    routing_keys = jax.random.split(jax.random.fold_in(key_of[14], 1), BATCH // SEQ_GRP)
    routing_turns = jax.random.permutation(jax.random.fold_in(key_of[14], 3), BATCH // SEQ_GRP)
    routing = jax.vmap(lambda own, number: assign_block(jax.random.fold_in(key_of[14], 2), own, number, SEQ_GRP, EXPERTS, TOPK, CAP, 2))(routing_keys, routing_turns).reshape((BATCH, TOPK))
    route_weight = jnp.clip(jnp.exp(math.log(1.0) - 2.3025851 * jax.random.uniform(key_of[15], (BATCH, TOPK), jnp.float32) ** steps_of(key_of[15], (BATCH, TOPK), ((0, 16),), -0.2, 0.2)), 0.1, 1.0)
    dense_gate = normal_values(key_of[16], (D, DFF_D), D ** -0.5, 0.125, ((1, 16),))
    dense_up = normal_values(key_of[17], (D, DFF_D), D ** -0.5, 0.125, ((1, 16),))
    dense_down = normal_values(key_of[18], (DFF_D, D), DFF_D ** -0.5, 0.125, ((0, 16),))
    mix_weight = normal_values(key_of[19], (D,), D ** -0.5, 0.125)
    second_gain = jnp.clip(1.0 + 0.18 * jax.random.normal(key_of[20], (D,), jnp.float32), 0.1, 1.9)
    return dict(tokens=tokens, conv_state=conv_state, rec_state=rec_state, gate_proj=gate_proj, input_proj=input_proj, conv_taps=conv_taps, decay_blocks=decay_blocks, input_blocks=input_blocks, decay_param=decay_param, out_proj=out_proj, first_gain=first_gain, expert_gate=expert_gate, expert_up=expert_up, expert_down=expert_down, routing=routing, route_weight=route_weight, dense_gate=dense_gate, dense_up=dense_up, dense_down=dense_down, mix_weight=mix_weight, second_gain=second_gain)


ALPHA = 8.0 ** 0.25
RATE_SCALE = 8.0
NORM_EPS = 1e-05

def norm_rows(values, gain_vec):
    centre = values - lax.optimization_barrier(jnp.mean(values, axis=-1, keepdims=True))
    spread = lax.optimization_barrier(jnp.mean(centre * centre, axis=-1, keepdims=True))
    return centre * lax.rsqrt(spread + NORM_EPS) * gain_vec

def split_dot(left, right, pieces):
    rows_count = left.shape[0]
    inner = left.shape[1]
    left_view = left.reshape(rows_count, pieces, inner // pieces).astype(jnp.float32)
    right_view = right.reshape(pieces, inner // pieces, right.shape[1]).astype(jnp.float32)
    partial_value = jnp.einsum('mpk,pkn->pmn', left_view, right_view)
    rounded = lax.optimization_barrier(partial_value.astype(jnp.bfloat16))
    return lax.optimization_barrier(jnp.sum(rounded.astype(jnp.float32), axis=0))

def reference(tokens, conv_state, rec_state, gate_proj, input_proj, conv_taps, decay_blocks, input_blocks, decay_param, out_proj, first_gain, expert_gate, expert_up, expert_down, routing, route_weight, dense_gate, dense_up, dense_down, mix_weight, second_gain):
    count_rows = tokens.shape[0]
    gated = jnp.dot(tokens, gate_proj, preferred_element_type=jnp.float32).astype(jnp.bfloat16)
    inputs = jnp.dot(tokens, input_proj, preferred_element_type=jnp.float32).astype(jnp.bfloat16)
    window = jnp.concatenate([conv_state, inputs[:, None, :]], axis=1)
    convolved = lax.optimization_barrier(jnp.sum(window.astype(jnp.float32) * conv_taps.astype(jnp.float32)[None], axis=1)).astype(jnp.bfloat16)
    heads_view = convolved.reshape(count_rows, HEADS, -1).astype(jnp.float32)
    recur_gate = jax.nn.sigmoid(jnp.einsum('bhi,hij->bhj', heads_view, decay_blocks.astype(jnp.float32))).reshape(count_rows, -1)
    input_gate = jax.nn.sigmoid(jnp.einsum('bhi,hij->bhj', heads_view, input_blocks.astype(jnp.float32))).reshape(count_rows, -1)
    log_decay = -RATE_SCALE * recur_gate * jax.nn.softplus(-decay_param)
    new_state = jnp.exp(log_decay) * rec_state + jnp.sqrt(-jnp.expm1(2.0 * log_decay)) * input_gate * convolved.astype(jnp.float32)
    mixed_rows = (new_state * jax.nn.gelu(gated.astype(jnp.float32), approximate=True)).astype(jnp.bfloat16)
    mixed = split_dot(mixed_rows, out_proj, N_TP)
    normed = norm_rows(ALPHA * tokens.astype(jnp.float32) + mixed, first_gain).astype(jnp.bfloat16)
    experts = expert_gate.shape[0]
    labels = jnp.arange(experts, dtype=jnp.int32)
    weight_table = jnp.zeros((count_rows, experts), jnp.float32)
    routed = jnp.zeros((count_rows, experts), jnp.int32)
    for which in range(TOPK):
        match = routing[:, which][:, None] == labels[None, :]
        weight_table = weight_table + jnp.where(match, route_weight[:, which][:, None], 0.0)
        routed = routed + match.astype(jnp.int32)
    positions = jnp.arange(count_rows, dtype=jnp.int32)
    sort_keys = jnp.where(routed.T > 0, positions[None, :], count_rows + positions[None, :])
    chosen = jnp.argsort(sort_keys, axis=1)[:, :N_EP * CAP].astype(jnp.int32)

    def one_expert(running, members):
        rows_index, weight_col, gate_mat, up_mat, down_mat = members
        rows_data = normed[rows_index]
        gate_val = jnp.dot(rows_data, gate_mat, preferred_element_type=jnp.float32)
        up_val = jnp.dot(rows_data, up_mat, preferred_element_type=jnp.float32)
        hidden = (jax.nn.silu(gate_val) * up_val).astype(jnp.bfloat16)
        result = split_dot(hidden, down_mat, N_TP).astype(jnp.bfloat16)
        running = running.at[rows_index].add(weight_col[rows_index][:, None] * result.astype(jnp.float32))
        return (running, None)
    routed_sum, unused = lax.scan(one_expert, jnp.zeros((count_rows, D), jnp.float32), (chosen, weight_table.T, expert_gate, expert_up, expert_down))
    dense_g = jnp.dot(normed, dense_gate, preferred_element_type=jnp.float32)
    dense_u = jnp.dot(normed, dense_up, preferred_element_type=jnp.float32)
    dense_hidden = (jax.nn.silu(dense_g) * dense_u).astype(jnp.bfloat16)
    dense_out = split_dot(dense_hidden, dense_down, N_TP)
    mix = jax.nn.sigmoid(jnp.dot(normed, mix_weight, preferred_element_type=jnp.float32))
    combined = ALPHA * normed.astype(jnp.float32) + routed_sum + mix[:, None] * dense_out
    layer_out = norm_rows(combined, second_gain).astype(jnp.bfloat16)
    return (layer_out, new_state, window[:, 1:])
```

```python
import functools

import jax
import jax.numpy as jnp
from jax import lax
from jax.experimental import pallas as pl
from jax.experimental.pallas import tpu as pltpu
from jax.sharding import PartitionSpec as P

MESH = pl.DeviceIdType.MESH
ALPHA = 8.0**0.25
RATE_SCALE = 8.0
NORM_EPS = 1e-05
TOPK = 2
F32 = jnp.float32
BF16 = jnp.bfloat16


def dot(a, b):
    return jnp.dot(a, b, preferred_element_type=F32)


def dot_nt(a, b):
    return lax.dot_general(a, b, (((1,), (1,)), ((), ())), preferred_element_type=F32)


def one_less_exp(u):
    series = 1.0 - u * (1.0 / 8.0)
    for k in (7, 6, 5, 4, 3, 2):
        series = 1.0 - u * (1.0 / k) * series
    return jnp.where(u < 0.5, u * series, 1.0 - jnp.exp(-u))


def kernel(
    nz, ny, nx, cap,
    tok_h, conv_r, rec_r, gp_h, ip_h, taps_r, db_r, ib_r, dp_r, op_h, fg_r,
    eg_h, eu_h, ed_h, rt_r, rw_r, dg_h, du_h, dd_h, mw_r, sg_r,
    lo_o, ns_o, nc_o,
    tok, gp, ip, op, eg, eu, ed, dg, du, dd,
    pm_s, pm_r, pm_own, zs, zr, st_s, st_r, nrm, onehot, wts, ds, xin,
    ps, pr, po, rs, ret, dps, dpr, dacc, fs, fr, ss, sr,
    w_sem, ed_sem, dd_sem,
    pm_sem, z_ssem, z_rsem, st_sem, ag_ssem, ag_rsem, fw_ssem, fw_rsem,
    dx_ssem, dx_rsem, fx_ssem, fx_rsem, po_ssem, po_rsem, rt_ssem, rt_rsem,
    dp_sem, f_ssem, f_rsem, s_ssem, s_rsem,
):
    ne, ntp = ny * nx, 2 * nz
    rows, d = tok.shape
    half = d // 2
    zr_rows = rows // nz
    ep, tp = lax.axis_index("ep"), lax.axis_index("tp")
    z, c = lax.div(tp, 2), lax.rem(tp, 2)
    oc = 1 - c
    y, x = lax.div(ep, nx), lax.rem(ep, nx)
    partner = {"ep": ep, "tp": 2 * z + oc}

    def zdev(k, core):
        return {"ep": ep, "tp": 2 * lax.rem(z + k + nz, nz) + core}

    def edev(dy, dx):
        return lax.rem(y + dy + ny, ny) * nx + lax.rem(x + dx + nx, nx)

    def remote(src, dst, ssem, rsem, dev):
        return pltpu.make_async_remote_copy(
            src_ref=src, dst_ref=dst, send_sem=ssem, recv_sem=rsem,
            device_id=dev, device_id_type=MESH,
        )

    barrier = pltpu.get_barrier_semaphore()
    greeted = 0
    for k in range(nz):
        for core in (c, oc):
            if k == 0 and core is c:
                continue
            pl.semaphore_signal(barrier, inc=1, device_id=zdev(k, core), device_id_type=MESH)
            greeted += 1
    for dy in range(ny):
        for dx in range(nx):
            if dy or dx:
                pl.semaphore_signal(
                    barrier, inc=1, device_id={"ep": edev(dy, dx), "tp": tp}, device_id_type=MESH
                )
                greeted += 1

    loads = {}
    for i, (name, src, dst) in enumerate((
        ("tok", tok_h, tok), ("gp", gp_h, gp), ("ip", ip_h, ip),
        ("op0", op_h.at[:, pl.ds(0, half)], op.at[0]),
        ("op1", op_h.at[:, pl.ds(half, half)], op.at[1]),
        ("dg", dg_h, dg), ("du", du_h, du), ("eg", eg_h, eg), ("eu", eu_h, eu),
    )):
        loads[name] = pltpu.make_async_copy(src, dst, w_sem.at[i])
        loads[name].start()
    for name, src, dst, sem in (("dd", dd_h, dd, dd_sem), ("ed", ed_h, ed, ed_sem)):
        parts = []
        for j in range(ntp):
            parts.append(pltpu.make_async_copy(
                src.at[:, pl.ds(128 * j, 128)],
                dst.at[j % 2, :, pl.ds(128 * (j // 2), 128)],
                sem.at[j],
            ))
            parts[-1].start()
        loads[name] = parts

    eids = lax.broadcasted_iota(jnp.int32, (ne, rows), 0)
    named = [rt_r[k : k + 1, :] == eids for k in range(TOPK)]
    either = jnp.where(named[0] | named[1], 1.0, 0.0)
    before = jnp.where(
        lax.broadcasted_iota(jnp.int32, (rows, rows), 0)
        < lax.broadcasted_iota(jnp.int32, (rows, rows), 1), 1.0, 0.0,
    )
    place = dot(either.astype(BF16), before.astype(BF16))
    slots = lax.broadcasted_iota(jnp.int32, (ne, cap, rows), 1).astype(F32)
    hit = (place[:, None, :] == slots) & (either[:, None, :] > 0.5)
    hot = jnp.where(hit, 1.0, 0.0)
    onehot[...] = hot.reshape(ny, nx * cap, rows).astype(BF16)
    weight = jnp.where(named[0], rw_r[0:1, :], 0.0) + jnp.where(named[1], rw_r[1:2, :], 0.0)
    weighted = (hot * weight[:, None, :]).reshape(ne * cap, rows).T
    upper = weighted.astype(BF16)
    wts[0:rows, :] = upper
    wts[rows:, :] = (weighted - upper.astype(F32)).astype(BF16)

    for name in ("tok", "gp", "ip"):
        loads[name].wait()
    gated = dot(tok[...], gp[...]).astype(BF16)
    inputs = dot(tok[...], ip[...]).astype(BF16)
    taps = taps_r[...].astype(F32)
    conv = inputs.astype(F32) * taps[3:4, :]
    for k in range(3):
        conv += conv_r[k].astype(F32) * taps[k : k + 1, :]
    nc_o[0] = conv_r[1]
    nc_o[1] = conv_r[2]
    nc_o[2] = inputs
    convolved = conv.astype(BF16)
    recur_gate = jax.nn.sigmoid(dot(convolved, db_r[0]))
    input_gate = jax.nn.sigmoid(dot(convolved, ib_r[0]))
    param = dp_r[...]
    soft = jnp.maximum(-param, 0.0) + jnp.log1p(jnp.exp(-jnp.abs(param)))
    log_decay = -RATE_SCALE * recur_gate * soft
    state = jnp.exp(log_decay) * rec_r[...] + jnp.sqrt(
        one_less_exp(-2.0 * log_decay)
    ) * input_gate * convolved.astype(F32)
    ns_o[...] = state
    g = gated.astype(F32)
    gelu = 0.5 * g * (1.0 + jnp.tanh(0.7978845608028654 * (g + 0.044715 * g * g * g)))
    mixed_rows = (state * gelu).astype(BF16)
    loads["op0"].wait()
    loads["op1"].wait()
    pm_s[...] = dot(mixed_rows, op[oc]).astype(BF16)

    pl.semaphore_wait(barrier, greeted)

    sent = []
    cp = remote(pm_s, pm_r, pm_sem.at[0], pm_sem.at[1], partner)
    cp.start()
    sent.append(cp)
    pm_own[...] = dot(mixed_rows, op[c])
    cp.wait_recv()
    zs[...] = (pm_own[...] + pm_r[...].astype(F32)).astype(BF16).reshape(nz, zr_rows, half)
    arrivals = []
    for k in range(1, nz):
        peer = lax.rem(z + k, nz)
        cp = remote(zs.at[peer], zr.at[z], z_ssem.at[k], z_rsem.at[k], zdev(k, c))
        cp.start()
        sent.append(cp)
        arrivals.append((k, cp))
    my_rows = pl.ds(pl.multiple_of(z * zr_rows, zr_rows), zr_rows)
    my_cols = pl.ds(pl.multiple_of(c * half, half), half)
    total = ALPHA * tok[my_rows, my_cols].astype(F32) + zs[z].astype(F32)
    for k, cp in arrivals:
        cp.wait_recv()
        total += zr[lax.rem(z - k + nz, nz)].astype(F32)
    row_sum = jnp.sum(total, axis=1, keepdims=True)
    row_mean = row_sum / half
    row_m2 = jnp.sum(jnp.square(total - row_mean), axis=1, keepdims=True)
    st_s[0] = jnp.broadcast_to(row_mean, (zr_rows, 128))
    st_s[1] = jnp.broadcast_to(row_m2, (zr_rows, 128))
    cp = remote(st_s, st_r, st_sem.at[0], st_sem.at[1], partner)
    cp.start()
    sent.append(cp)
    cp.wait_recv()
    peer_mean, peer_m2 = st_r[0][:, 0:1], st_r[1][:, 0:1]
    mean = 0.5 * (row_mean + peer_mean)
    variance = (row_m2 + peer_m2 + jnp.square(row_mean - peer_mean) * (half / 2)) / d
    nrm[c, z] = (
        (total - mean) * lax.rsqrt(variance + NORM_EPS) * fg_r[:, my_cols]
    ).astype(BF16)

    arrivals = []
    for k in range(1, nz):
        cp = remote(nrm.at[c, z], nrm.at[c, z], ag_ssem.at[k], ag_rsem.at[k], zdev(k, c))
        cp.start()
        sent.append(cp)
        arrivals.append((k, cp))
    handed = []
    cp = remote(nrm.at[c, z], nrm.at[c, z], fw_ssem.at[0], fw_rsem.at[0], partner)
    cp.start()
    sent.append(cp)
    handed.append(cp)
    for k, cp in arrivals:
        cp.wait_recv()
        src = lax.rem(z - k + nz, nz)
        cp = remote(nrm.at[c, src], nrm.at[c, src], fw_ssem.at[k], fw_rsem.at[k], partner)
        cp.start()
        sent.append(cp)
        handed.append(cp)

    mine = nrm[c].reshape(rows, half)
    group = nx * cap
    arrivals = {}
    for dy in range(ny):
        yy = lax.rem(y + dy, ny)
        ds[pl.ds(yy * nx, nx)] = dot(onehot[yy], mine).astype(BF16).reshape(nx, cap, half)
        for dx in range(nx):
            e = edev(dy, dx)
            i = dy * nx + dx
            if i:
                cp = remote(
                    ds.at[e], xin.at[c, ep], dx_ssem.at[i], dx_rsem.at[i], {"ep": e, "tp": tp}
                )
                cp.start()
                sent.append(cp)
                arrivals[i] = cp

    for cp in handed:
        cp.wait_recv()
    n0, n1 = nrm[0].reshape(rows, half), nrm[1].reshape(rows, half)
    loads["dg"].wait()
    loads["du"].wait()
    dense_g = dot(n0, dg[0:half, :]) + dot(n1, dg[half:, :])
    dense_u = dot(n0, du[0:half, :]) + dot(n1, du[half:, :])
    dense_hidden = (jax.nn.silu(dense_g) * dense_u).astype(BF16)
    for cp in loads["dd"]:
        cp.wait()
    dps[...] = dot(dense_hidden, dd[oc]).astype(BF16)
    dense_swap = remote(dps, dpr, dp_sem.at[0], dp_sem.at[1], partner)
    dense_swap.start()
    sent.append(dense_swap)
    dacc[...] = dot(dense_hidden, dd[c])
    mixing = jnp.sum(n0.astype(F32) * mw_r[:, 0:half].astype(F32), axis=1, keepdims=True)
    mixing += jnp.sum(n1.astype(F32) * mw_r[:, half:].astype(F32), axis=1, keepdims=True)
    mix = jax.nn.sigmoid(mixing)
    dense_swap.wait_recv()
    dacc[...] = mix * (dacc[...] + dpr[...].astype(F32))

    loads["eg"].wait()
    loads["eu"].wait()
    for cp in loads["ed"]:
        cp.wait()
    returned = []

    def finish(dy):
        swap = swaps[dy]
        swap.wait_recv()
        yy = lax.rem(y - dy + ny, ny)
        rs[dy] = (po[dy] + pr[dy].astype(F32)).astype(BF16).reshape(nx, cap, half)
        for dx in range(nx):
            i = dy * nx + dx
            xx = lax.rem(x - dx + nx, nx)
            if i:
                cp = remote(
                    rs.at[dy, xx], ret.at[ep], rt_ssem.at[i], rt_rsem.at[i],
                    {"ep": yy * nx + xx, "tp": tp},
                )
                cp.start()
                sent.append(cp)
                returned.append(cp)
            else:
                ret[ep] = rs[dy, xx]

    swaps = []
    for dy in range(ny):
        yy = lax.rem(y - dy + ny, ny)
        handed = []
        for dx in range(nx):
            i = dy * nx + dx
            src = yy * nx + lax.rem(x - dx + nx, nx)
            if i:
                arrivals[i].wait_recv()
            else:
                xin[c, ep] = ds[ep]
            cp = remote(xin.at[c, src], xin.at[c, src], fx_ssem.at[i], fx_rsem.at[i], partner)
            cp.start()
            sent.append(cp)
            handed.append(cp)
        if dy:
            finish(dy - 1)
        for cp in handed:
            cp.wait_recv()
        x0 = xin[0, pl.ds(yy * nx, nx)].reshape(group, half)
        x1 = xin[1, pl.ds(yy * nx, nx)].reshape(group, half)
        gate = dot_nt(x0, eg[:, 0:half]) + dot_nt(x1, eg[:, half:])
        up = dot_nt(x0, eu[:, 0:half]) + dot_nt(x1, eu[:, half:])
        hidden = (jax.nn.silu(gate) * up).astype(BF16)
        ps[dy] = dot(hidden, ed[oc]).astype(BF16)
        swap = remote(ps.at[dy], pr.at[dy], po_ssem.at[dy], po_rsem.at[dy], partner)
        swap.start()
        sent.append(swap)
        swaps.append(swap)
        po[dy] = dot(hidden, ed[c])
    finish(ny - 1)

    for cp in returned:
        cp.wait_recv()
    both = dot(wts[...], ret[...].reshape(ne * cap, half))
    dacc[...] += both[0:rows] + both[rows:]
    for k in range(nz):
        fs[k] = dacc[:, 128 * k : 128 * (k + 1)].astype(BF16)
    arrivals = []
    for k in range(1, nz):
        cp = remote(fs.at[lax.rem(z + k, nz)], fr.at[z], f_ssem.at[k], f_rsem.at[k], zdev(k, c))
        cp.start()
        sent.append(cp)
        arrivals.append((k, cp))
    column = pl.ds(pl.multiple_of(lax.rem(tp, nz) * 128, 128), 128)
    combined = ALPHA * nrm[lax.div(tp, nz), :, :, column].reshape(rows, 128).astype(F32)
    combined += fs[z].astype(F32)
    for k, cp in arrivals:
        cp.wait_recv()
        combined += fr[lax.rem(z - k + nz, nz)].astype(F32)

    turned = combined.T
    block_mean = jnp.sum(turned, axis=0, keepdims=True) / 128
    block_m2 = jnp.sum(jnp.square(turned - block_mean), axis=0, keepdims=True)
    ss[...] = jnp.concatenate(
        [block_mean, block_m2, jnp.zeros((6, rows), F32)], axis=0
    )
    arrivals = []
    for k in range(nz):
        for j, core in enumerate((c, oc)):
            if k or j:
                i = 2 * k + j
                cp = remote(ss, sr.at[i], s_ssem.at[i], s_rsem.at[i], zdev(k, core))
                cp.start()
                sent.append(cp)
                arrivals.append((i, cp))
    stats = [ss[...]]
    for i, cp in arrivals:
        cp.wait_recv()
        stats.append(sr[i])
    mean = sum(s[0:1] for s in stats) / ntp
    m2 = sum(s[1:2] + 128 * jnp.square(s[0:1] - mean) for s in stats)
    scaled = ((turned - mean) * lax.rsqrt(m2 / d + NORM_EPS)).T
    lo_o[...] = (scaled * sg_r[...]).astype(BF16)
    for cp in sent:
        cp.wait_send()


def on_device(
    nz, ny, nx,
    tokens, conv_state, rec_state, gate_proj, input_proj, conv_taps, decay_blocks, input_blocks,
    decay_param, out_proj, first_gain, expert_gate, expert_up, expert_down, routing, route_weight,
    dense_gate, dense_up, dense_down, mix_weight, second_gain,
):
    rows, d = tokens.shape
    half = d // 2
    ne, ntp = ny * nx, 2 * nz
    cap = max(2, 2 * rows * TOPK // ne)
    group = nx * cap
    ff = expert_gate.shape[2]
    zrow = rows // nz
    vmem, hbm = pl.BlockSpec(memory_space=pltpu.VMEM), pl.BlockSpec(memory_space=pl.ANY)
    dma = pltpu.SemaphoreType.DMA
    args = [
        (tokens, hbm), (conv_state.transpose(1, 0, 2), vmem), (rec_state, vmem),
        (gate_proj, hbm), (input_proj, hbm), (conv_taps, vmem), (decay_blocks, vmem),
        (input_blocks, vmem), (decay_param.reshape(1, -1), vmem), (out_proj, hbm),
        (first_gain.reshape(1, -1), vmem), (expert_gate[0].T, hbm), (expert_up[0].T, hbm),
        (expert_down[0], hbm), (routing.T, vmem), (route_weight.T, vmem), (dense_gate, hbm),
        (dense_up, hbm), (dense_down, hbm), (mix_weight.reshape(1, -1), vmem),
        (second_gain.reshape(1, -1), vmem),
    ]
    scratch = [
        ((rows, d), BF16), ((d, 128), BF16), ((d, 128), BF16), ((2, rows, half), BF16),
        ((ff, d), BF16), ((ff, d), BF16), ((2, ff, half), BF16),
        ((d, 128), BF16), ((d, 128), BF16), ((2, 128, half), BF16),
        ((rows, half), BF16), ((rows, half), BF16), ((rows, half), F32),
        ((nz, zrow, half), BF16), ((nz, zrow, half), BF16),
        ((2, zrow, 128), F32), ((2, zrow, 128), F32),
        ((2, nz, zrow, half), BF16), ((ny, group, rows), BF16), ((2 * rows, ne * cap), BF16),
        ((ne, cap, half), BF16), ((2, ne, cap, half), BF16),
        ((ny, group, half), BF16), ((ny, group, half), BF16), ((ny, group, half), F32),
        ((ny, nx, cap, half), BF16), ((ne, cap, half), BF16),
        ((rows, half), BF16), ((rows, half), BF16), ((rows, half), F32),
        ((nz, rows, 128), BF16), ((nz, rows, 128), BF16),
        ((8, rows), F32), ((ntp, 8, rows), F32),
    ]
    sems = [9, ntp, ntp, 2, nz, nz, 2, nz, nz, nz, nz, ne, ne, ne, ne, ny, ny, ne, ne, 2, nz, nz, ntp, ntp]
    layer_out, new_state, new_conv = pl.pallas_call(
        functools.partial(kernel, nz, ny, nx, cap),
        name="decode_step",
        out_shape=(
            jax.ShapeDtypeStruct((rows, 128), BF16),
            jax.ShapeDtypeStruct((rows, 128), F32),
            jax.ShapeDtypeStruct((3, rows, 128), BF16),
        ),
        in_specs=[spec for _, spec in args],
        out_specs=(vmem, vmem, vmem),
        scratch_shapes=[pltpu.VMEM(*s) for s in scratch] + [dma((n,)) for n in sems],
        compiler_params=pltpu.CompilerParams(collective_id=0, has_side_effects=True),
    )(*[a for a, _ in args])
    return layer_out, new_state, new_conv.transpose(1, 0, 2)


def solution(mesh):
    ep, tp = mesh.shape["ep"], mesh.shape["tp"]
    ny = nx = 4 if ep == 16 else 2
    return jax.shard_map(
        functools.partial(on_device, tp // 2, ny, nx),
        mesh=mesh,
        in_specs=(
            P("ep", None), P("ep", None, "tp"), P("ep", "tp"), P(None, "tp"), P(None, "tp"),
            P(None, "tp"), P("tp", None, None), P("tp", None, None), P("tp"), P("tp", None), P(),
            P("ep", None, "tp"), P("ep", None, "tp"), P("ep", "tp", None), P("ep", None),
            P("ep", None), P(None, "tp"), P(None, "tp"), P("tp", None), P(), P("tp"),
        ),
        out_specs=(P("ep", "tp"), P("ep", "tp"), P("ep", None, "tp")),
        check_vma=False,
    )
```

```python
import functools

import jax
import jax.numpy as jnp
from jax import lax
from jax.experimental import pallas as pl
from jax.experimental.pallas import tpu as pltpu
from jax.sharding import PartitionSpec as P

MESH = pl.DeviceIdType.MESH
ALPHA = 8.0**0.25
RATE_SCALE = 8.0
NORM_EPS = 1e-05
TOPK = 2
F32 = jnp.float32
BF16 = jnp.bfloat16


def dot(a, b):
    return jnp.dot(a, b, preferred_element_type=F32)


def dot_nt(a, b):
    return lax.dot_general(a, b, (((1,), (1,)), ((), ())), preferred_element_type=F32)


def one_less_exp(u):
    series = 1.0 - u * (1.0 / 8.0)
    for k in (7, 6, 5, 4, 3, 2):
        series = 1.0 - u * (1.0 / k) * series
    return jnp.where(u < 0.5, u * series, 1.0 - jnp.exp(-u))


def kernel(nz, ny, nx, cap, names, *refs):
    hbm = dict(zip(names["args"], refs))
    refs = refs[len(hbm) :]
    lo_o, ns_o, nc_o = refs[:3]
    v = dict(zip(names["scratch"], refs[3:]))
    sem = dict(zip(names["sems"], refs[3 + len(v) :]))

    tok = v["tokens"]
    ne, ntp = ny * nx, 2 * nz
    rows, d = tok.shape
    half, quarter = d // 2, d // 4
    zrow, hz, hx = rows // nz, nz // 2, nx // 2
    group = nx * cap
    ep, tp = lax.axis_index("ep"), lax.axis_index("tp")
    z, c = lax.div(tp, 2), lax.rem(tp, 2)
    oc, q = 1 - c, lax.rem(z, 2)
    y, x = lax.div(ep, nx), lax.rem(ep, nx)
    partner = {"ep": ep, "tp": 2 * z + oc}

    def zdev(k, core):
        return {"ep": ep, "tp": 2 * lax.rem(z + k + nz, nz) + core}

    def edev(dy, dx):
        return lax.rem(y + dy + ny, ny) * nx + lax.rem(x + dx + nx, nx)

    sent = []

    def send(src, dst, name, i, dev):
        copy = pltpu.make_async_remote_copy(
            src_ref=src, dst_ref=dst,
            send_sem=sem[name + "_s"].at[i], recv_sem=sem[name + "_r"].at[i],
            device_id=dev, device_id_type=MESH,
        )
        copy.start()
        sent.append(copy)
        return copy

    barrier = pltpu.get_barrier_semaphore()
    greeted = 0
    for k in range(nz):
        for j, core in enumerate((c, oc)):
            if k or j:
                pl.semaphore_signal(barrier, inc=1, device_id=zdev(k, core), device_id_type=MESH)
                greeted += 1
    for dy in range(ny):
        for dx in range(nx):
            if dy or dx:
                pl.semaphore_signal(
                    barrier, inc=1, device_id={"ep": edev(dy, dx), "tp": tp}, device_id_type=MESH
                )
                greeted += 1

    loads = {}

    def load(name, pieces):
        for src, dst in pieces:
            i = len([1 for copies in loads.values() for _ in copies])
            copy = pltpu.make_async_copy(src, dst, sem["load"].at[i])
            copy.start()
            loads.setdefault(name, []).append(copy)

    def arrived(*wanted):
        for name in wanted:
            for copy in loads[name]:
                copy.wait()

    for name in (
        "tokens", "input_proj", "gate_proj", "conv_taps", "conv_state", "decay_blocks",
        "input_blocks", "decay_param", "rec_state", "routing", "route_weight",
    ):
        load(name, [(hbm[name], v[name])])
    load("out_proj", [
        (hbm["out_proj"].at[:, pl.ds(half * j, half)], v["out_proj"].at[j]) for j in range(2)
    ])
    load("first_gain", [(hbm["first_gain"], v["first_gain"])])
    starts = [
        (rel, core, pl.multiple_of(core * half + lax.rem(q + rel, 2) * quarter, quarter))
        for rel in range(2) for core in range(2)
    ]
    for name in ("dense_gate", "dense_up"):
        load(name, [
            (hbm[name].at[pl.ds(at, quarter), :], v[name].at[rel, core])
            for rel, core, at in starts
        ])
    for name in ("expert_gate", "expert_up"):
        load(name, [
            (hbm[name].at[:, pl.ds(at, quarter)], v[name].at[rel, core])
            for rel, core, at in starts
        ])
    for name in ("dense_down", "expert_down"):
        load(name, [
            (
                hbm[name].at[:, pl.ds(128 * j, 128)],
                v[name].at[j % 2, (j // 2) % 2, :, pl.ds(128 * (j // 4), 128)],
            )
            for j in range(ntp)
        ])
    for name in ("mix_weight", "second_gain"):
        load(name, [(hbm[name], v[name])])

    arrived("tokens", "input_proj")
    inputs = dot(tok[...], v["input_proj"][...]).astype(BF16)
    arrived("gate_proj")
    gated = dot(tok[...], v["gate_proj"][...]).astype(BF16)
    arrived("conv_taps", "conv_state", "decay_blocks", "input_blocks", "decay_param", "rec_state")
    taps = v["conv_taps"][...].astype(F32)
    conv = inputs.astype(F32) * taps[3:4, :]
    for k in range(3):
        conv += v["conv_state"][k].astype(F32) * taps[k : k + 1, :]
    convolved = conv.astype(BF16)
    recur_gate = jax.nn.sigmoid(dot(convolved, v["decay_blocks"][0]))
    input_gate = jax.nn.sigmoid(dot(convolved, v["input_blocks"][0]))
    param = v["decay_param"][...]
    soft = jnp.maximum(-param, 0.0) + jnp.log1p(jnp.exp(-jnp.abs(param)))
    log_decay = -RATE_SCALE * recur_gate * soft
    state = jnp.exp(log_decay) * v["rec_state"][...] + jnp.sqrt(
        one_less_exp(-2.0 * log_decay)
    ) * input_gate * convolved.astype(F32)
    g = gated.astype(F32)
    gelu = 0.5 * g * (1.0 + jnp.tanh(0.7978845608028654 * (g + 0.044715 * g * g * g)))
    mixed_rows = (state * gelu).astype(BF16)
    arrived("out_proj")
    v["pm_s"][...] = dot(mixed_rows, v["out_proj"][oc]).astype(BF16)

    pl.semaphore_wait(barrier, greeted)

    swap = send(v["pm_s"], v["pm_r"], "pm", 0, partner)
    v["pm_own"][...] = dot(mixed_rows, v["out_proj"][c])
    v["state"][...] = state
    v["window"][0] = v["conv_state"][1]
    v["window"][1] = v["conv_state"][2]
    v["window"][2] = inputs
    stores = [
        pltpu.make_async_copy(v["state"], ns_o, sem["store"].at[0]),
        pltpu.make_async_copy(v["window"], nc_o, sem["store"].at[1]),
    ]
    for copy in stores:
        copy.start()
    swap.wait_recv()
    v["zs"][...] = (v["pm_own"][...] + v["pm_r"][...].astype(F32)).astype(BF16).reshape(
        nz, zrow, half
    )
    copies = [
        (k, send(v["zs"].at[lax.rem(z + k, nz)], v["zr"].at[z], "z", k, zdev(k, c)))
        for k in range(1, nz)
    ]

    arrived("routing", "route_weight", "first_gain")
    routes, route_weight = v["routing"][...], v["route_weight"][...]
    eids = lax.broadcasted_iota(jnp.int32, (ne, rows), 0)
    named = [routes[k : k + 1, :] == eids for k in range(TOPK)]
    either = jnp.where(named[0] | named[1], 1.0, 0.0)
    before = jnp.where(
        lax.broadcasted_iota(jnp.int32, (rows, rows), 0)
        < lax.broadcasted_iota(jnp.int32, (rows, rows), 1), 1.0, 0.0,
    )
    place = dot(either.astype(BF16), before.astype(BF16))
    slots = lax.broadcasted_iota(jnp.int32, (ne, cap, rows), 1).astype(F32)
    hit = (place[:, None, :] == slots) & (either[:, None, :] > 0.5)
    hot = jnp.where(hit, 1.0, 0.0)
    v["onehot"][...] = hot.reshape(ny, group, rows).astype(BF16)
    weight = jnp.where(named[0], route_weight[0:1, :], 0.0)
    weight += jnp.where(named[1], route_weight[1:2, :], 0.0)
    weighted = (hot * weight[:, None, :]).reshape(ne * cap, rows).T
    upper = weighted.astype(BF16)
    v["wts"][0:rows, :] = upper
    v["wts"][rows:, :] = (weighted - upper.astype(F32)).astype(BF16)

    my_rows = pl.ds(pl.multiple_of(z * zrow, zrow), zrow)
    my_cols = pl.ds(pl.multiple_of(c * half, half), half)
    total = ALPHA * tok[my_rows, my_cols].astype(F32) + v["zs"][z].astype(F32)
    for k, copy in copies:
        copy.wait_recv()
        total += v["zr"][lax.rem(z - k + nz, nz)].astype(F32)

    row_mean = jnp.sum(total, axis=1, keepdims=True) / half
    row_m2 = jnp.sum(jnp.square(total - row_mean), axis=1, keepdims=True)
    v["st_s"][0] = jnp.broadcast_to(row_mean, (zrow, 128))
    v["st_s"][1] = jnp.broadcast_to(row_m2, (zrow, 128))
    send(v["st_s"], v["st_r"], "st", 0, partner).wait_recv()
    peer_mean, peer_m2 = v["st_r"][0][:, 0:1], v["st_r"][1][:, 0:1]
    mean = 0.5 * (row_mean + peer_mean)
    variance = (row_m2 + peer_m2 + jnp.square(row_mean - peer_mean) * (half / 2)) / d
    normed = (
        (total - mean) * lax.rsqrt(variance + NORM_EPS) * v["first_gain"][:, my_cols]
    ).astype(BF16)
    first, second = normed[:, 0:quarter], normed[:, quarter:]
    even = q == 0
    nrm = v["nrm"]
    v["nother"][...] = jnp.where(even, second, first)
    nrm[0, c, z] = jnp.where(even, first, second)

    copies = [
        send(v["nother"] if k % 2 else nrm.at[0, c, z], nrm.at[0, c, z], "ag", k, zdev(k, c))
        for k in range(1, nz)
    ]
    for copy in copies:
        copy.wait_recv()

    mine = nrm[0, c].reshape(rows, quarter)
    xin, ds = v["xin"], v["ds"]
    out_copies = {}
    for dy in range(ny):
        yy = lax.rem(y + dy, ny)
        block = dot(v["onehot"][yy], mine).astype(BF16).reshape(nx, cap, quarter)
        if dy:
            ds[pl.ds(yy * nx, nx)] = block
        else:
            ds[pl.ds(yy * nx, nx)] = block
            xin[0, c, ep] = ds[ep]
        for dx in range(nx):
            e, i = edev(dy, dx), dy * nx + dx
            if i:
                out_copies[i] = send(ds.at[e], xin.at[0, c, ep], "dx", i, {"ep": e, "tp": tp})

    first_z, last_z = pl.ds(0, hz), pl.ds(hz, hz)
    beside = [
        send(nrm.at[0, c, part], nrm.at[1, c, part], "nz", j, zdev(k, c))
        for j, (part, k) in enumerate(((first_z, 1), (last_z, -1)))
    ]
    handed = [send(nrm.at[0, c], nrm.at[0, c], "np", 0, partner)]
    for copy in beside:
        copy.wait_recv()
    handed.append(send(nrm.at[1, c], nrm.at[1, c], "np", 1, partner))

    state_of = {}

    def source_row(dy):
        return lax.rem(y - dy + ny, ny)

    def arrive(dy):
        yy = source_row(dy)
        for dx in range(nx):
            if dy or dx:
                out_copies[dy * nx + dx].wait_recv()
        whole = pl.ds(yy * nx, nx)
        parts = (pl.ds(yy * nx, hx), 1), (pl.ds(yy * nx + hx, hx), -1)
        state_of["z", dy] = [
            send(xin.at[0, c, part], xin.at[1, c, part], "xz", 2 * dy + j, zdev(k, c))
            for j, (part, k) in enumerate(parts)
        ]
        state_of["pair", dy] = [
            send(xin.at[0, c, whole], xin.at[0, c, whole], "xp", 2 * dy, partner)
        ]

    def hand_over(dy):
        for copy in state_of["z", dy]:
            copy.wait_recv()
        whole = pl.ds(source_row(dy) * nx, nx)
        state_of["pair", dy].append(
            send(xin.at[1, c, whole], xin.at[1, c, whole], "xp", 2 * dy + 1, partner)
        )

    def compute(dy):
        for copy in state_of["pair", dy]:
            copy.wait_recv()
        whole = pl.ds(source_row(dy) * nx, nx)
        gate = up = None
        for rel in range(2):
            for core in range(2):
                piece = xin[rel, core, whole].reshape(group, quarter)
                more = dot_nt(piece, v["expert_gate"][rel, core])
                gate = more if gate is None else gate + more
                more = dot_nt(piece, v["expert_up"][rel, core])
                up = more if up is None else up + more
        hidden = (jax.nn.silu(gate) * up).astype(BF16)
        for j, par in enumerate((1 - q, q)):
            v["ps"][dy, j] = dot(hidden, v["expert_down"][oc, par]).astype(BF16)
        state_of["sum", dy] = send(v["ps"].at[dy], v["pr"].at[dy], "po", dy, partner)
        for j, par in enumerate((1 - q, q)):
            v["po"][dy, j] = dot(hidden, v["expert_down"][c, par])

    def pair_sum(dy):
        state_of["sum", dy].wait_recv()
        v["bs"][dy] = (v["po"][dy, 0] + v["pr"][dy, 0].astype(F32)).astype(BF16)
        mid = group // 2
        parts = (pl.ds(0, mid), 1), (pl.ds(mid, mid), -1)
        state_of["beside", dy] = [
            send(v["bs"].at[dy, part], v["br"].at[dy, part], "bz", 2 * dy + j, zdev(k, c))
            for j, (part, k) in enumerate(parts)
        ]

    returned = []

    def go_home(dy):
        for copy in state_of["beside", dy]:
            copy.wait_recv()
        yy = source_row(dy)
        v["rs"][dy] = (
            v["po"][dy, 1] + v["pr"][dy, 1].astype(F32) + v["br"][dy].astype(F32)
        ).astype(BF16).reshape(nx, cap, quarter)
        for dx in range(nx):
            xx = lax.rem(x - dx + nx, nx)
            if dy or dx:
                returned.append(send(
                    v["rs"].at[dy, xx], v["ret"].at[ep], "rt", dy * nx + dx,
                    {"ep": yy * nx + xx, "tp": tp},
                ))
            else:
                v["ret"][ep] = v["rs"][dy, xx]

    def dense_start():
        arrived("dense_gate", "dense_up", "dense_down", "mix_weight")
        for copy in handed:
            copy.wait_recv()
        gate = up = mixing = None
        v["mixf"][...] = v["mix_weight"][...].astype(F32)
        for rel, core, _ in starts:
            piece = nrm[rel, core].reshape(rows, quarter)
            more = dot(piece, v["dense_gate"][rel, core])
            gate = more if gate is None else gate + more
            more = dot(piece, v["dense_up"][rel, core])
            up = more if up is None else up + more
            for j in range(quarter // 128):
                at = (core * 2 + lax.rem(q + rel, 2)) * (quarter // 128) + j
                more = piece[:, 128 * j : 128 * (j + 1)].astype(F32) * v["mixf"][pl.ds(at, 1), :]
                mixing = more if mixing is None else mixing + more
        hidden = (jax.nn.silu(gate) * up).astype(BF16)
        for j, par in enumerate((1 - q, q)):
            v["dps"][j] = dot(hidden, v["dense_down"][oc, par]).astype(BF16)
            v["dpo"][j] = dot(hidden, v["dense_down"][c, par])
        v["mix"][...] = jnp.broadcast_to(
            jax.nn.sigmoid(jnp.sum(mixing, axis=1, keepdims=True)), (rows, 128)
        )
        state_of["dense"] = send(v["dps"], v["dpr"], "dp", 0, partner)

    def dense_pair():
        state_of["dense"].wait_recv()
        v["dbs"][...] = (v["dpo"][0] + v["dpr"][0].astype(F32)).astype(BF16)
        mid = rows // 2
        parts = (pl.ds(0, mid), 1), (pl.ds(mid, mid), -1)
        state_of["dense_beside"] = [
            send(v["dbs"].at[part], v["dbr"].at[part], "db", j, zdev(k, c))
            for j, (part, k) in enumerate(parts)
        ]

    def dense_end():
        for copy in state_of["dense_beside"]:
            copy.wait_recv()
        v["dacc"][...] = v["mix"][:, 0:1] * (
            v["dpo"][1] + v["dpr"][1].astype(F32) + v["dbr"][...].astype(F32)
        )

    def experts_loaded():
        arrived("expert_gate", "expert_up", "expert_down")

    plan = [(arrive, 0), (dense_start,), (arrive, 1), (hand_over, 0), (experts_loaded,), (compute, 0),
            (dense_pair,), (arrive, 2), (hand_over, 1), (pair_sum, 0), (compute, 1), (dense_end,),
            (arrive, 3), (hand_over, 2), (go_home, 0), (pair_sum, 1), (compute, 2), (hand_over, 3),
            (go_home, 1), (pair_sum, 2), (compute, 3), (go_home, 2), (pair_sum, 3), (go_home, 3)]
    for step, *which in plan:
        if not which or which[0] < ny:
            step(*which)

    for copy in returned:
        copy.wait_recv()
    both = dot(v["wts"][...], v["ret"][...].reshape(ne * cap, quarter))
    fin = v["dacc"][...] + both[0:rows] + both[rows:]
    for k in range(hz):
        v["fs"][k] = fin[:, 128 * k : 128 * (k + 1)].astype(BF16)
    zh = lax.div(z, 2)
    copies = [
        (k, send(v["fs"].at[lax.rem(zh + k, hz)], v["fr"].at[zh], "f", k, zdev(2 * k, c)))
        for k in range(1, hz)
    ]
    place_of = lax.rem(tp, nz)
    column = pl.ds(pl.multiple_of(lax.rem(place_of, hz) * 128, 128), 128)
    own = nrm[lax.rem(lax.div(place_of, hz) + q, 2), lax.div(tp, nz), :, :, column]
    combined = ALPHA * own.reshape(rows, 128).astype(F32) + v["fs"][zh].astype(F32)
    for k, copy in copies:
        copy.wait_recv()
        combined += v["fr"][lax.rem(zh - k + hz, hz)].astype(F32)

    arrived("second_gain")
    turned = combined.T
    block_mean = jnp.sum(turned, axis=0, keepdims=True) / 128
    block_m2 = jnp.sum(jnp.square(turned - block_mean), axis=0, keepdims=True)
    v["ss"][...] = jnp.concatenate([block_mean, block_m2, jnp.zeros((6, rows), F32)], axis=0)
    copies = [
        (2 * k + j, send(v["ss"], v["sr"].at[2 * k + j], "s", 2 * k + j, zdev(k, core)))
        for k in range(nz) for j, core in enumerate((c, oc)) if k or j
    ]
    stats = [v["ss"][...]]
    for i, copy in copies:
        copy.wait_recv()
        stats.append(v["sr"][i])
    mean = sum(s[0:1] for s in stats) / ntp
    m2 = sum(s[1:2] + 128 * jnp.square(s[0:1] - mean) for s in stats)
    scaled = ((turned - mean) * lax.rsqrt(m2 / d + NORM_EPS)).T
    v["out"][...] = (scaled * v["second_gain"][...]).astype(BF16)
    stores.append(pltpu.make_async_copy(v["out"], lo_o, sem["store"].at[2]))
    stores[-1].start()
    for copy in sent:
        copy.wait_send()
    for copy in stores:
        copy.wait()


def hand_out(*refs):
    arrays, sem = refs[:9], refs[9]
    moves = [
        [pltpu.make_async_copy(arrays[i], arrays[6 + i], sem.at[i]) for i in range(3)],
        [pltpu.make_async_copy(arrays[6 + i], arrays[3 + i], sem.at[3 + i]) for i in range(3)],
    ]
    for copy in moves[0]:
        copy.start()
    for into, out in zip(*moves):
        into.wait()
        out.start()
    for copy in moves[1]:
        copy.wait()


def on_device(nz, ny, nx, *arrays):
    names = (
        "tokens conv_state rec_state gate_proj input_proj conv_taps decay_blocks input_blocks"
        " decay_param out_proj first_gain expert_gate expert_up expert_down routing route_weight"
        " dense_gate dense_up dense_down mix_weight second_gain"
    ).split()
    args = dict(zip(names, arrays))
    rows, d = args["tokens"].shape
    ff = args["expert_gate"].shape[2]
    args["conv_state"] = args["conv_state"].transpose(1, 0, 2)
    for name in ("decay_param", "first_gain", "second_gain"):
        args[name] = args[name].reshape(1, -1)
    for name in ("expert_gate", "expert_up"):
        args[name] = args[name][0].T
    args["expert_down"] = args["expert_down"][0]
    args["routing"], args["route_weight"] = args["routing"].T, args["route_weight"].T
    args["mix_weight"] = args["mix_weight"].reshape(-1, 128)

    half, quarter = d // 2, d // 4
    ne, ntp, hz = ny * nx, 2 * nz, nz // 2
    cap = max(2, 2 * rows * TOPK // ne)
    group, zrow = nx * cap, rows // nz
    scratch = {name: (a.shape, a.dtype) for name, a in args.items()}
    scratch.update(
        out_proj=((2, rows, half), BF16),
        expert_gate=((2, 2, ff, quarter), BF16), expert_up=((2, 2, ff, quarter), BF16),
        expert_down=((2, 2, ff, quarter), BF16),
        dense_gate=((2, 2, quarter, 128), BF16), dense_up=((2, 2, quarter, 128), BF16),
        dense_down=((2, 2, 128, quarter), BF16),
        pm_s=((rows, half), BF16), pm_r=((rows, half), BF16), pm_own=((rows, half), F32),
        state=((rows, 128), F32), window=((3, rows, 128), BF16), out=((rows, 128), BF16),
        zs=((nz, zrow, half), BF16), zr=((nz, zrow, half), BF16),
        st_s=((2, zrow, 128), F32), st_r=((2, zrow, 128), F32),
        nrm=((2, 2, nz, zrow, quarter), BF16), nother=((zrow, quarter), BF16),
        onehot=((ny, group, rows), BF16), wts=((2 * rows, ne * cap), BF16),
        ds=((ne, cap, quarter), BF16), xin=((2, 2, ne, cap, quarter), BF16),
        ps=((ny, 2, group, quarter), BF16), pr=((ny, 2, group, quarter), BF16),
        po=((ny, 2, group, quarter), F32),
        bs=((ny, group, quarter), BF16), br=((ny, group, quarter), BF16),
        rs=((ny, nx, cap, quarter), BF16), ret=((ne, cap, quarter), BF16),
        mixf=((d // 128, 128), F32), mix=((rows, 128), F32),
        dps=((2, rows, quarter), BF16), dpr=((2, rows, quarter), BF16),
        dpo=((2, rows, quarter), F32), dbs=((rows, quarter), BF16), dbr=((rows, quarter), BF16),
        dacc=((rows, quarter), F32),
        fs=((hz, rows, 128), BF16), fr=((hz, rows, 128), BF16),
        ss=((8, rows), F32), sr=((ntp, 8, rows), F32),
    )
    pairs = dict(
        pm=1, z=nz, st=1, ag=nz, np=2, nz=2, dx=ne, xz=2 * ny, xp=2 * ny, po=ny, bz=2 * ny, rt=ne,
        dp=1, db=2, f=hz, s=ntp,
    )
    sems = {"load": 32 + 2 * ntp, "store": 3}
    for name, n in pairs.items():
        sems[name + "_s"] = sems[name + "_r"] = n
    anywhere = pl.BlockSpec(memory_space=pl.ANY)
    outs = (
        jax.ShapeDtypeStruct((rows, 128), BF16),
        jax.ShapeDtypeStruct((rows, 128), F32),
        jax.ShapeDtypeStruct((3, rows, 128), BF16),
    )
    labels = {"args": tuple(args), "scratch": tuple(scratch), "sems": tuple(sems)}
    results = pl.pallas_call(
        functools.partial(kernel, nz, ny, nx, cap, labels),
        name="decode_step",
        out_shape=outs,
        in_specs=[anywhere] * len(args),
        out_specs=(anywhere,) * 3,
        scratch_shapes=[pltpu.VMEM(*s) for s in scratch.values()]
        + [pltpu.SemaphoreType.DMA((n,)) for n in sems.values()],
        compiler_params=pltpu.CompilerParams(collective_id=0, has_side_effects=True),
    )(*args.values())
    layer_out, new_state, new_conv = pl.pallas_call(
        hand_out,
        name="hand_out",
        out_shape=outs,
        in_specs=[anywhere] * 3,
        out_specs=(anywhere,) * 3,
        scratch_shapes=[pltpu.VMEM(s.shape, s.dtype) for s in outs]
        + [pltpu.SemaphoreType.DMA((6,))],
    )(*results)
    return layer_out, new_state, new_conv.transpose(1, 0, 2)


def solution(mesh):
    ep, tp = mesh.shape["ep"], mesh.shape["tp"]
    nx = {16: 4, 4: 2, 2: 2}[ep]
    return jax.shard_map(
        functools.partial(on_device, tp // 2, ep // nx, nx),
        mesh=mesh,
        in_specs=(
            P("ep", None), P("ep", None, "tp"), P("ep", "tp"), P(None, "tp"), P(None, "tp"),
            P(None, "tp"), P("tp", None, None), P("tp", None, None), P("tp"), P("tp", None), P(),
            P("ep", None, "tp"), P("ep", None, "tp"), P("ep", "tp", None), P("ep", None),
            P("ep", None), P(None, "tp"), P(None, "tp"), P("tp", None), P(), P("tp"),
        ),
        out_specs=(P("ep", "tp"), P("ep", "tp"), P("ep", None, "tp")),
        check_vma=False,
    )
```

```python
import functools
from types import SimpleNamespace
from typing import Any, NamedTuple

import jax
import jax.numpy as jnp
from jax import lax
from jax.experimental import pallas as pl
from jax.experimental.pallas import tpu as pltpu
from jax.sharding import PartitionSpec as P

MESH = pl.DeviceIdType.MESH
ALPHA = 8.0**0.25
RATE_SCALE = 8.0
NORM_EPS = 1e-05
TOPK = 2
F32 = jnp.float32
BF16 = jnp.bfloat16


class Args(NamedTuple):
    tokens: Any
    conv_state: Any
    rec_state: Any
    gate_proj: Any
    input_proj: Any
    conv_taps: Any
    decay_blocks: Any
    input_blocks: Any
    decay_param: Any
    out_proj: Any
    first_gain: Any
    expert_gate: Any
    expert_up: Any
    expert_down: Any
    routing: Any
    route_weight: Any
    dense_gate: Any
    dense_up: Any
    dense_down: Any
    mix_weight: Any
    second_gain: Any


def dot(a, b):
    return jnp.dot(a, b, preferred_element_type=F32)


def dot_nt(a, b):
    return lax.dot_general(a, b, (((1,), (1,)), ((), ())), preferred_element_type=F32)


def one_less_exp(u):
    series = 1.0 - u * (1.0 / 8.0)
    for k in (7, 6, 5, 4, 3, 2):
        series = 1.0 - u * (1.0 / k) * series
    return jnp.where(u < 0.5, u * series, 1.0 - jnp.exp(-u))


def kernel(nz, ny, nx, cap, names, *refs):
    hbm = Args(*refs[: len(Args._fields)])
    refs = refs[len(hbm) :]
    lo_o, ns_o, nc_o = refs[:3]
    v = SimpleNamespace(**dict(zip(names[0], refs[3:])))
    sem = dict(zip(names[1], refs[3 + len(names[0]) :]))

    tok = v.tokens
    ne, ntp = ny * nx, 2 * nz
    rows, d = tok.shape
    half, quarter = d // 2, d // 4
    zrow, hz, group = rows // nz, nz // 2, nx * cap
    ep, tp = lax.axis_index("ep"), lax.axis_index("tp")
    z, c = lax.div(tp, 2), lax.rem(tp, 2)
    oc, q = 1 - c, lax.rem(z, 2)
    y, x = lax.div(ep, nx), lax.rem(ep, nx)
    partner = {"ep": ep, "tp": 2 * z + oc}

    def zdev(k, core):
        return {"ep": ep, "tp": 2 * lax.rem(z + k + nz, nz) + core}

    def edev(dy, dx):
        return lax.rem(y + dy + ny, ny) * nx + lax.rem(x + dx + nx, nx)

    def send(src, dst, name, i, dev):
        copy = pltpu.make_async_remote_copy(
            src_ref=src, dst_ref=dst,
            send_sem=sem[name + "_s"].at[0], recv_sem=sem[name + "_r"].at[i],
            device_id=dev, device_id_type=MESH,
        )
        copy.start()
        return copy

    def whole(ref, name, i=0):
        return pltpu.make_async_remote_copy(
            src_ref=ref, dst_ref=ref,
            send_sem=sem[name + "_s"].at[0], recv_sem=sem[name + "_r"].at[i],
            device_id=partner, device_id_type=MESH,
        )

    barrier = pltpu.get_barrier_semaphore()
    greeted = 0
    for k in range(nz):
        for j, core in enumerate((c, oc)):
            if k or j:
                pl.semaphore_signal(barrier, inc=1, device_id=zdev(k, core), device_id_type=MESH)
                greeted += 1
    for dy in range(ny):
        for dx in range(nx):
            if dy or dx:
                pl.semaphore_signal(
                    barrier, inc=1, device_id={"ep": edev(dy, dx), "tp": tp}, device_id_type=MESH
                )
                greeted += 1

    loads = {}

    def load(dst, *pieces):
        at = sem["load"].at[len(loads)]
        loads[id(dst)] = pltpu.make_async_copy(dst, dst, at)
        for src, part in pieces:
            pltpu.make_async_copy(src, part, at).start()

    def arrived(*wanted):
        for dst in wanted:
            loads[id(dst)].wait()

    for dst, src in (
        (v.tokens, hbm.tokens), (v.input_proj, hbm.input_proj), (v.gate_proj, hbm.gate_proj),
        (v.conv_taps, hbm.conv_taps), (v.conv_state, hbm.conv_state),
        (v.decay_blocks, hbm.decay_blocks), (v.input_blocks, hbm.input_blocks),
        (v.decay_param, hbm.decay_param), (v.rec_state, hbm.rec_state),
    ):
        load(dst, (src, dst))
    load(v.out_proj, *[
        (hbm.out_proj.at[:, pl.ds(half * j, half)], v.out_proj.at[j]) for j in range(2)
    ])
    for dst, src in (
        (v.routing, hbm.routing), (v.route_weight, hbm.route_weight),
        (v.first_gain, hbm.first_gain),
    ):
        load(dst, (src, dst))
    starts = [
        (rel, core, pl.multiple_of(core * half + lax.rem(q + rel, 2) * quarter, quarter))
        for rel in range(2) for core in range(2)
    ]
    for dst, src in (v.dense_gate, hbm.dense_gate), (v.dense_up, hbm.dense_up):
        load(dst, *[
            (src.at[pl.ds(at, quarter), :], dst.at[rel, core]) for rel, core, at in starts
        ])
    for dst, src in (v.expert_gate, hbm.expert_gate), (v.expert_up, hbm.expert_up):
        load(dst, *[
            (src.at[:, pl.ds(at, quarter)], dst.at[rel, core]) for rel, core, at in starts
        ])
    for dst, src in (v.dense_down, hbm.dense_down), (v.expert_down, hbm.expert_down):
        load(dst, *[
            (
                src.at[:, pl.ds(128 * j, 128)],
                dst.at[j % 2, (j // 2) % 2, :, pl.ds(128 * (j // 4), 128)],
            )
            for j in range(ntp)
        ])
    for dst, src in (v.mix_weight, hbm.mix_weight), (v.second_gain, hbm.second_gain):
        load(dst, (src, dst))

    arrived(v.tokens, v.input_proj)
    inputs = dot(tok[...], v.input_proj[...]).astype(BF16)
    arrived(v.gate_proj)
    gated = dot(tok[...], v.gate_proj[...]).astype(BF16)
    arrived(v.conv_taps, v.conv_state, v.decay_blocks, v.input_blocks, v.decay_param, v.rec_state)
    taps = v.conv_taps[...].astype(F32)
    conv = inputs.astype(F32) * taps[3:4, :]
    for k in range(3):
        conv += v.conv_state[k].astype(F32) * taps[k : k + 1, :]
    convolved = conv.astype(BF16)
    recur_gate = jax.nn.sigmoid(dot(convolved, v.decay_blocks[0]))
    input_gate = jax.nn.sigmoid(dot(convolved, v.input_blocks[0]))
    param = v.decay_param[...]
    soft = jnp.maximum(-param, 0.0) + jnp.log1p(jnp.exp(-jnp.abs(param)))
    log_decay = -RATE_SCALE * recur_gate * soft
    state = jnp.exp(log_decay) * v.rec_state[...] + jnp.sqrt(
        one_less_exp(-2.0 * log_decay)
    ) * input_gate * convolved.astype(F32)
    g = gated.astype(F32)
    gelu = 0.5 * g * (1.0 + jnp.tanh(0.7978845608028654 * (g + 0.044715 * g * g * g)))
    mixed_rows = (state * gelu).astype(BF16)
    arrived(v.out_proj)
    v.pm_s[...] = dot(mixed_rows, v.out_proj[oc]).astype(BF16)

    pl.semaphore_wait(barrier, greeted)

    swap = send(v.pm_s, v.pm_r, "pm", 0, partner)
    v.pm_own[...] = dot(mixed_rows, v.out_proj[c])
    v.state[...] = state
    v.window[0] = v.conv_state[1]
    v.window[1] = v.conv_state[2]
    v.window[2] = inputs
    stores = [
        pltpu.make_async_copy(v.state, ns_o, sem["store"].at[0]),
        pltpu.make_async_copy(v.window, nc_o, sem["store"].at[1]),
    ]
    for copy in stores:
        copy.start()
    swap.wait_recv()
    v.zs[...] = (v.pm_own[...] + v.pm_r[...].astype(F32)).astype(BF16).reshape(
        nz, zrow, half
    )
    for k in range(1, nz):
        send(v.zs.at[lax.rem(z + k, nz)], v.zr.at[z], "z", 0, zdev(k, c))

    arrived(v.routing, v.route_weight, v.first_gain)
    routes, route_weight = v.routing[...], v.route_weight[...]
    eids = lax.broadcasted_iota(jnp.int32, (ne, rows), 0)
    named = [routes[k : k + 1, :] == eids for k in range(TOPK)]
    either = jnp.where(named[0] | named[1], 1.0, 0.0)
    before = jnp.where(
        lax.broadcasted_iota(jnp.int32, (rows, rows), 0)
        < lax.broadcasted_iota(jnp.int32, (rows, rows), 1), 1.0, 0.0,
    )
    place = dot(either.astype(BF16), before.astype(BF16))
    slots = lax.broadcasted_iota(jnp.int32, (ne, cap, rows), 1).astype(F32)
    hit = (place[:, None, :] == slots) & (either[:, None, :] > 0.5)
    hot = jnp.where(hit, 1.0, 0.0)
    v.onehot[...] = hot.reshape(ny, group, rows).astype(BF16)
    weight = jnp.where(named[0], route_weight[0:1, :], 0.0)
    weight += jnp.where(named[1], route_weight[1:2, :], 0.0)
    weighted = (hot * weight[:, None, :]).reshape(ne * cap, rows).T
    upper = weighted.astype(BF16)
    v.wts[0:rows, :] = upper
    v.wts[rows:, :] = (weighted - upper.astype(F32)).astype(BF16)

    my_rows = pl.ds(pl.multiple_of(z * zrow, zrow), zrow)
    my_cols = pl.ds(pl.multiple_of(c * half, half), half)
    total = ALPHA * tok[my_rows, my_cols].astype(F32) + v.zs[z].astype(F32)
    whole(v.zr.at[pl.ds(0, nz - 1)], "z").wait_recv()
    for k in range(1, nz):
        total += v.zr[lax.rem(z - k + nz, nz)].astype(F32)

    row_mean = jnp.sum(total, axis=1, keepdims=True) / half
    row_m2 = jnp.sum(jnp.square(total - row_mean), axis=1, keepdims=True)
    v.st_s[0] = jnp.broadcast_to(row_mean, (zrow, 128))
    v.st_s[1] = jnp.broadcast_to(row_m2, (zrow, 128))
    send(v.st_s, v.st_r, "st", 0, partner).wait_recv()
    peer_mean, peer_m2 = v.st_r[0][:, 0:1], v.st_r[1][:, 0:1]
    mean = 0.5 * (row_mean + peer_mean)
    variance = (row_m2 + peer_m2 + jnp.square(row_mean - peer_mean) * (half / 2)) / d
    normed = (
        (total - mean) * lax.rsqrt(variance + NORM_EPS) * v.first_gain[:, my_cols]
    ).astype(BF16)
    first, second = normed[:, 0:quarter], normed[:, quarter:]
    even = q == 0
    nrm = v.nrm
    v.nother[...] = jnp.where(even, second, first)
    nrm[0, c, z] = jnp.where(even, first, second)

    for k in range(1, nz):
        send(v.nother if k % 2 else nrm.at[0, c, z], nrm.at[0, c, z], "ag", 0, zdev(k, c))
    whole(nrm.at[0, c, pl.ds(0, nz - 1)], "ag").wait_recv()

    xin, ds = v.xin, v.ds
    offsets = [(dy, dx) for dy in range(ny) for dx in range(nx)]
    if ny == nx == 4:
        offsets = [
            (2, 2), (3, 2), (2, 3), (2, 1), (1, 2), (3, 1), (1, 3), (2, 0),
            (0, 2), (3, 3), (1, 1), (3, 0), (1, 0), (0, 3), (0, 1), (0, 0),
        ]
    last = ny - 1

    def members(f):
        return list(enumerate(offsets))[f * nx : (f + 1) * nx]

    def dispatch(f, rel, out, name, at, done):
        for p, (dy, dx) in members(f):
            yy, e = lax.rem(y + dy, ny), edev(dy, dx)
            if dy not in done:
                done.add(dy)
                out[pl.ds(yy * nx, nx)] = dot(
                    v.onehot[yy], nrm[rel, c].reshape(rows, quarter)
                ).astype(BF16).reshape(nx, cap, quarter)
        for p, (dy, dx) in members(f):
            if dy or dx:
                e = edev(dy, dx)
                send(out.at[e], xin.at[rel, c, p], name, at, {"ep": e, "tp": tp})
            else:
                xin[rel, c, p] = out[ep]

    done = set()
    for f in range(ny):
        dispatch(f, 0, ds, "dx", f, done)

    first_z, last_z = pl.ds(0, hz), pl.ds(hz, hz)
    for part, k in (first_z, 1), (last_z, -1):
        send(nrm.at[0, c, part], nrm.at[1, c, part], "nz", 0, zdev(k, c))
    send(nrm.at[0, c], nrm.at[0, c], "np", 0, partner)

    per = min(2, ny)
    flight = {}

    def halves(src, dst, count, name, at):
        for part, k in (pl.ds(0, count // 2), 1), (pl.ds(count // 2, count // 2), -1):
            send(src.at[part], dst.at[part], name, at, zdev(k, c))
        return whole(dst, name, at)

    def normed_beside(_):
        whole(nrm.at[1, c], "nz").wait_recv()
        send(nrm.at[1, c], nrm.at[1, c], "np", 0, partner)
        dispatch(last, 1, v.ds2, "d2", 0, set())

    def arrive(f):
        count = len([p for p, at in members(f) if at != (0, 0)])
        whole(xin.at[0, c, pl.ds(f * nx, count)], "dx", f).wait_recv()
        row = pl.ds(f * nx, nx)
        if f != last:
            flight["z", f] = halves(xin.at[0, c, row], xin.at[1, c, row], nx, "xz", f)
        flight["own", f] = send(xin.at[0, c, row], xin.at[0, c, row], "xp", 2 * f, partner)

    def hand_over(f):
        if f != last:
            flight["z", f].wait_recv()
        else:
            count = len([p for p, at in members(f) if at != (0, 0)])
            whole(xin.at[1, c, pl.ds(f * nx, count)], "d2").wait_recv()
        row = pl.ds(f * nx, nx)
        flight["other", f] = send(xin.at[1, c, row], xin.at[1, c, row], "xp", 2 * f + 1, partner)

    def gate_up(k, rel):
        pieces = [
            xin[rel, core, pl.ds(k * per * nx, per * nx)].reshape(per * group, quarter)
            for core in range(2)
        ]
        return [
            dot_nt(pieces[0], weights[rel, 0]) + dot_nt(pieces[1], weights[rel, 1])
            for weights in (v.expert_gate, v.expert_up)
        ]

    def compute_own(k):
        if k == 0:
            arrived(v.expert_gate, v.expert_up)
        for f in range(k * per, (k + 1) * per):
            flight["own", f].wait_recv()
        v.gate[k], v.up[k] = gate_up(k, 0)

    def compute_other(k):
        for f in range(k * per, (k + 1) * per):
            flight["other", f].wait_recv()
        gate, up = gate_up(k, 1)
        v.hidden[k] = (jax.nn.silu(v.gate[k] + gate) * (v.up[k] + up)).astype(BF16)

    def down(k):
        fine = range(k * per, (k + 1) * per)
        if k == 0:
            arrived(v.expert_down)
        hidden = v.hidden[k]
        for j, par in enumerate((1 - q, q)):
            product = dot(hidden, v.expert_down[oc, par]).astype(BF16)
            for f in fine:
                at = (f - k * per) * group
                v.ps[f, j] = product[at : at + group]
                flight["sum", f, j] = send(
                    v.ps.at[f, j], v.pr.at[f, j], "po", 2 * f + j, partner
                )
        for j, par in enumerate((1 - q, q)):
            product = dot(hidden, v.expert_down[c, par])
            for f in fine:
                at = (f - k * per) * group
                v.po[f, j] = product[at : at + group]

    def pair_sum(f):
        flight["sum", f, 0].wait_recv()
        v.bs[f] = (v.po[f, 0] + v.pr[f, 0].astype(F32)).astype(BF16)
        flight["beside", f] = halves(v.bs.at[f], v.br.at[f], group, "bz", f)

    def go_home(f):
        flight["sum", f, 1].wait_recv()
        flight["beside", f].wait_recv()
        v.rs[pl.ds(f * nx, nx)] = (
            v.po[f, 1] + v.pr[f, 1].astype(F32) + v.br[f].astype(F32)
        ).astype(BF16).reshape(nx, cap, quarter)
        for p, (dy, dx) in members(f):
            if dy or dx:
                home = {"ep": edev(-dy, -dx), "tp": tp}
                send(v.rs.at[p], v.ret.at[ep], "rt", 0, home)
            else:
                v.ret[ep] = v.rs[p]

    def dense_start(_):
        arrived(v.dense_gate, v.dense_up, v.dense_down, v.mix_weight)
        whole(nrm.at[:, c], "np").wait_recv()
        gate = up = mixing = None
        v.mixf[...] = v.mix_weight[...].astype(F32)
        for rel, core, _ in starts:
            piece = nrm[rel, core].reshape(rows, quarter)
            more = dot(piece, v.dense_gate[rel, core])
            gate = more if gate is None else gate + more
            more = dot(piece, v.dense_up[rel, core])
            up = more if up is None else up + more
            for j in range(quarter // 128):
                at = (core * 2 + lax.rem(q + rel, 2)) * (quarter // 128) + j
                more = piece[:, 128 * j : 128 * (j + 1)].astype(F32) * v.mixf[pl.ds(at, 1), :]
                mixing = more if mixing is None else mixing + more
        hidden = (jax.nn.silu(gate) * up).astype(BF16)
        for j, par in enumerate((1 - q, q)):
            v.dps[j] = dot(hidden, v.dense_down[oc, par]).astype(BF16)
        flight["dense"] = send(v.dps, v.dpr, "dp", 0, partner)
        for j, par in enumerate((1 - q, q)):
            v.dpo[j] = dot(hidden, v.dense_down[c, par])
        v.mix[...] = jnp.broadcast_to(
            jax.nn.sigmoid(jnp.sum(mixing, axis=1, keepdims=True)), (rows, 128)
        )

    def dense_pair(_):
        flight["dense"].wait_recv()
        v.dbs[...] = (v.dpo[0] + v.dpr[0].astype(F32)).astype(BF16)
        flight["dense_beside"] = halves(v.dbs, v.dbr, rows, "db", 0)

    def dense_end(_):
        flight["dense_beside"].wait_recv()
        v.dacc[...] = v.mix[:, 0:1] * (
            v.dpo[1] + v.dpr[1].astype(F32) + v.dbr[...].astype(F32)
        )

    plan = [
        (normed_beside, 0), (arrive, 0), (arrive, 1), (arrive, 2), (dense_start, 0), (arrive, 3),
        (hand_over, 0), (compute_own, 0), (hand_over, 1), (hand_over, 3), (compute_own, 1),
        (compute_other, 0), (hand_over, 2), (down, 0), (compute_other, 1), (pair_sum, 0),
        (pair_sum, 1), (down, 1), (pair_sum, 2), (pair_sum, 3), (dense_pair, 0), (go_home, 0),
        (go_home, 1), (go_home, 2), (go_home, 3), (dense_end, 0),
    ]
    for step, which in plan:
        if which < (ny // per if step in (compute_own, compute_other, down) else ny):
            step(which)

    whole(v.ret.at[pl.ds(0, ne - 1)], "rt").wait_recv()
    both = dot(v.wts[...], v.ret[...].reshape(ne * cap, quarter))
    fin = v.dacc[...] + both[0:rows] + both[rows:]
    for k in range(hz):
        v.fs[k] = fin[:, 128 * k : 128 * (k + 1)].astype(BF16)
    zh = lax.div(z, 2)
    for k in range(1, hz):
        send(v.fs.at[lax.rem(zh + k, hz)], v.fr.at[zh], "f", 0, zdev(2 * k, c))
    place_of = lax.rem(tp, nz)
    column = pl.ds(pl.multiple_of(lax.rem(place_of, hz) * 128, 128), 128)
    own = nrm[lax.rem(lax.div(place_of, hz) + q, 2), lax.div(tp, nz), :, :, column]
    combined = ALPHA * own.reshape(rows, 128).astype(F32) + v.fs[zh].astype(F32)
    if hz > 1:
        whole(v.fr.at[pl.ds(0, hz - 1)], "f").wait_recv()
    for k in range(1, hz):
        combined += v.fr[lax.rem(zh - k + hz, hz)].astype(F32)

    arrived(v.second_gain)
    turned = combined.T
    block_mean = jnp.sum(turned, axis=0, keepdims=True) / 128
    block_m2 = jnp.sum(jnp.square(turned - block_mean), axis=0, keepdims=True)
    v.ss[...] = jnp.concatenate([block_mean, block_m2, jnp.zeros((6, rows), F32)], axis=0)
    peers = [(k, core, 2 * k + j) for k in range(nz) for j, core in enumerate((c, oc)) if k or j]
    for k, core, i in peers:
        send(v.ss, v.sr.at[i], "s", 0, zdev(k, core))
    whole(v.sr.at[pl.ds(0, ntp - 1)], "s").wait_recv()
    stats = [v.ss[...]] + [v.sr[i] for _, _, i in peers]
    mean = sum(s[0:1] for s in stats) / ntp
    m2 = sum(s[1:2] + 128 * jnp.square(s[0:1] - mean) for s in stats)
    scaled = ((turned - mean) * lax.rsqrt(m2 / d + NORM_EPS)).T
    v.out[...] = (scaled * v.second_gain[...]).astype(BF16)
    stores.append(pltpu.make_async_copy(v.out, lo_o, sem["store"].at[2]))
    stores[-1].start()
    for name, ref in (
        ("pm", v.pm_s), ("z", v.zs.at[pl.ds(0, nz - 1)]), ("st", v.st_s),
        ("ag", nrm.at[0, c, pl.ds(0, nz - 1)]), ("np", nrm.at[:, c]), ("nz", nrm.at[0, c]),
        ("dx", ds.at[pl.ds(0, ne - 1)]), ("xz", xin.at[0, c, pl.ds(0, last * nx)]),
        ("d2", xin.at[0, c, pl.ds(0, len([p for p, at in members(last) if at != (0, 0)]))]), ("xp", xin.at[:, c]),
        ("po", v.ps), ("bz", v.bs), ("rt", v.rs.at[pl.ds(0, ne - 1)]), ("dp", v.dps),
        ("db", v.dbs), ("f", v.fs.at[pl.ds(0, hz - 1)]), ("s", v.sr.at[pl.ds(0, ntp - 1)]),
    ):
        if 0 not in ref.shape:
            whole(ref, name).wait_send()
    for copy in stores:
        copy.wait()


def hand_out(*refs):
    arrays, sem = refs[:9], refs[9]
    moves = [
        [pltpu.make_async_copy(arrays[i], arrays[6 + i], sem.at[i]) for i in range(3)],
        [pltpu.make_async_copy(arrays[6 + i], arrays[3 + i], sem.at[3 + i]) for i in range(3)],
    ]
    for copy in moves[0]:
        copy.start()
    for into, out in zip(*moves):
        into.wait()
        out.start()
    for copy in moves[1]:
        copy.wait()


def on_device(nz, ny, nx, *arrays):
    args = Args(*arrays)
    rows, d = args.tokens.shape
    ff = args.expert_gate.shape[2]
    args = args._replace(
        conv_state=args.conv_state.transpose(1, 0, 2),
        decay_param=args.decay_param.reshape(1, -1),
        first_gain=args.first_gain.reshape(1, -1),
        second_gain=args.second_gain.reshape(1, -1),
        expert_gate=args.expert_gate[0].T,
        expert_up=args.expert_up[0].T,
        expert_down=args.expert_down[0],
        routing=args.routing.T,
        route_weight=args.route_weight.T,
        mix_weight=args.mix_weight.reshape(-1, 128),
    )

    half, quarter = d // 2, d // 4
    ne, ntp, hz = ny * nx, 2 * nz, nz // 2
    cap = max(2, 2 * rows * TOPK // ne)
    group, zrow = nx * cap, rows // nz
    rows_at_once = min(2, ny) * group
    ng = ne * cap // rows_at_once
    scratch = {name: (a.shape, a.dtype) for name, a in args._asdict().items()}
    scratch.update(
        out_proj=((2, rows, half), BF16),
        expert_gate=((2, 2, ff, quarter), BF16), expert_up=((2, 2, ff, quarter), BF16),
        expert_down=((2, 2, ff, quarter), BF16),
        dense_gate=((2, 2, quarter, 128), BF16), dense_up=((2, 2, quarter, 128), BF16),
        dense_down=((2, 2, 128, quarter), BF16),
        pm_s=((rows, half), BF16), pm_r=((rows, half), BF16), pm_own=((rows, half), F32),
        state=((rows, 128), F32), window=((3, rows, 128), BF16), out=((rows, 128), BF16),
        zs=((nz, zrow, half), BF16), zr=((nz, zrow, half), BF16),
        st_s=((2, zrow, 128), F32), st_r=((2, zrow, 128), F32),
        nrm=((2, 2, nz, zrow, quarter), BF16), nother=((zrow, quarter), BF16),
        onehot=((ny, group, rows), BF16), wts=((2 * rows, ne * cap), BF16),
        ds=((ne, cap, quarter), BF16), ds2=((ne, cap, quarter), BF16),
        hidden=((ng, rows_at_once, ff), BF16), xin=((2, 2, ne, cap, quarter), BF16),
        ps=((ny, 2, group, quarter), BF16), pr=((ny, 2, group, quarter), BF16),
        po=((ny, 2, group, quarter), F32), gate=((ng, rows_at_once, ff), F32),
        up=((ng, rows_at_once, ff), F32),
        bs=((ny, group, quarter), BF16), br=((ny, group, quarter), BF16),
        rs=((ne, cap, quarter), BF16), ret=((ne, cap, quarter), BF16),
        mixf=((d // 128, 128), F32), mix=((rows, 128), F32),
        dps=((2, rows, quarter), BF16), dpr=((2, rows, quarter), BF16),
        dpo=((2, rows, quarter), F32), dbs=((rows, quarter), BF16), dbr=((rows, quarter), BF16),
        dacc=((rows, quarter), F32),
        fs=((hz, rows, 128), BF16), fr=((hz, rows, 128), BF16),
        ss=((8, rows), F32), sr=((ntp, 8, rows), F32),
    )
    pairs = dict(
        pm=1, z=1, st=1, ag=1, np=1, nz=1, dx=ny, d2=1, xz=ny, xp=2 * ny, po=2 * ny, bz=ny, rt=1, dp=1,
        db=1, f=1, s=1,
    )
    sems = {"load": len(args), "store": 3}
    for name, n in pairs.items():
        sems[name + "_s"], sems[name + "_r"] = 1, n
    anywhere = pl.BlockSpec(memory_space=pl.ANY)
    outs = (
        jax.ShapeDtypeStruct((rows, 128), BF16),
        jax.ShapeDtypeStruct((rows, 128), F32),
        jax.ShapeDtypeStruct((3, rows, 128), BF16),
    )
    labels = tuple(scratch), tuple(sems)
    results = pl.pallas_call(
        functools.partial(kernel, nz, ny, nx, cap, labels),
        name="decode_step",
        out_shape=outs,
        in_specs=[anywhere] * len(args),
        out_specs=(anywhere,) * 3,
        scratch_shapes=[pltpu.VMEM(*s) for s in scratch.values()]
        + [pltpu.SemaphoreType.DMA((n,)) for n in sems.values()],
        compiler_params=pltpu.CompilerParams(collective_id=0, has_side_effects=True),
    )(*args)
    layer_out, new_state, new_conv = pl.pallas_call(
        hand_out,
        name="hand_out",
        out_shape=outs,
        in_specs=[anywhere] * 3,
        out_specs=(anywhere,) * 3,
        scratch_shapes=[pltpu.VMEM(s.shape, s.dtype) for s in outs]
        + [pltpu.SemaphoreType.DMA((6,))],
    )(*results)
    return layer_out, new_state, new_conv.transpose(1, 0, 2)


def solution(mesh):
    ep, tp = mesh.shape["ep"], mesh.shape["tp"]
    nx = {16: 4, 4: 2, 2: 2}[ep]
    return jax.shard_map(
        functools.partial(on_device, tp // 2, ep // nx, nx),
        mesh=mesh,
        in_specs=(
            P("ep", None), P("ep", None, "tp"), P("ep", "tp"), P(None, "tp"), P(None, "tp"),
            P(None, "tp"), P("tp", None, None), P("tp", None, None), P("tp"), P("tp", None), P(),
            P("ep", None, "tp"), P("ep", None, "tp"), P("ep", "tp", None), P("ep", None),
            P("ep", None), P(None, "tp"), P(None, "tp"), P("tp", None), P(), P("tp"),
        ),
        out_specs=(P("ep", "tp"), P("ep", "tp"), P("ep", None, "tp")),
        check_vma=False,
    )
```

```python
import functools
from types import SimpleNamespace
from typing import Any, NamedTuple

import jax
import jax.numpy as jnp
from jax import lax
from jax.experimental import pallas as pl
from jax.experimental.pallas import tpu as pltpu
from jax.sharding import PartitionSpec as P

MESH = pl.DeviceIdType.MESH
ALPHA = 8.0**0.25
RATE_SCALE = 8.0
NORM_EPS = 1e-05
TOPK = 2
F32 = jnp.float32
BF16 = jnp.bfloat16


class Args(NamedTuple):
    tokens: Any
    conv_state: Any
    rec_state: Any
    gate_proj: Any
    input_proj: Any
    conv_taps: Any
    decay_blocks: Any
    input_blocks: Any
    decay_param: Any
    out_proj: Any
    first_gain: Any
    expert_gate: Any
    expert_up: Any
    expert_down: Any
    routing: Any
    route_weight: Any
    dense_gate: Any
    dense_up: Any
    dense_down: Any
    mix_weight: Any
    second_gain: Any


def dot(a, b):
    return jnp.dot(a, b, preferred_element_type=F32)


def dot_nt(a, b):
    return lax.dot_general(a, b, (((1,), (1,)), ((), ())), preferred_element_type=F32)


def one_less_exp(u):
    series = 1.0 - u * (1.0 / 8.0)
    for k in (7, 6, 5, 4, 3, 2):
        series = 1.0 - u * (1.0 / k) * series
    return jnp.where(u < 0.5, u * series, 1.0 - jnp.exp(-u))


def kernel(nz, ny, nx, cap, names, *refs):
    hbm = Args(*refs[: len(Args._fields)])
    refs = refs[len(hbm) :]
    lo_o, ns_o, nc_o = refs[:3]
    v = SimpleNamespace(**dict(zip(names[0], refs[3:])))
    sem = dict(zip(names[1], refs[3 + len(names[0]) :]))

    tok = v.tokens
    ne, ntp = ny * nx, 2 * nz
    rows, d = tok.shape
    half, quarter = d // 2, d // 4
    zrow, hz, group = rows // nz, nz // 2, nx * cap
    ep, tp = lax.axis_index("ep"), lax.axis_index("tp")
    z, c = lax.div(tp, 2), lax.rem(tp, 2)
    oc, q = 1 - c, lax.rem(z, 2)
    y, x = lax.div(ep, nx), lax.rem(ep, nx)
    partner = {"ep": ep, "tp": 2 * z + oc}

    def zdev(k, core):
        return {"ep": ep, "tp": 2 * lax.rem(z + k + nz, nz) + core}

    def edev(dy, dx):
        return lax.rem(y + dy + ny, ny) * nx + lax.rem(x + dx + nx, nx)

    def send(src, dst, name, i, dev):
        copy = pltpu.make_async_remote_copy(
            src_ref=src, dst_ref=dst,
            send_sem=sem[name + "_s"].at[0], recv_sem=sem[name + "_r"].at[i],
            device_id=dev, device_id_type=MESH,
        )
        copy.start()
        return copy

    def whole(ref, name, i=0):
        return pltpu.make_async_remote_copy(
            src_ref=ref, dst_ref=ref,
            send_sem=sem[name + "_s"].at[0], recv_sem=sem[name + "_r"].at[i],
            device_id=partner, device_id_type=MESH,
        )

    far_first = sorted(range(1, nz), key=lambda k: -min(k, nz - k))

    barrier = pltpu.get_barrier_semaphore()
    greeted = 0
    for k in far_first + [0]:
        for j, core in enumerate((c, oc)):
            if k or j:
                pl.semaphore_signal(barrier, inc=1, device_id=zdev(k, core), device_id_type=MESH)
                greeted += 1
    for dy in range(ny):
        for dx in range(nx):
            if dy or dx:
                pl.semaphore_signal(
                    barrier, inc=1, device_id={"ep": edev(dy, dx), "tp": tp}, device_id_type=MESH
                )
                greeted += 1

    loads = {}

    def load(dst, *pieces):
        at = sem["load"].at[len(loads)]
        loads[id(dst)] = pltpu.make_async_copy(dst, dst, at)
        for src, part in pieces:
            pltpu.make_async_copy(src, part, at).start()

    def arrived(*wanted):
        for dst in wanted:
            loads[id(dst)].wait()

    for dst, src in (
        (v.tokens, hbm.tokens), (v.input_proj, hbm.input_proj), (v.gate_proj, hbm.gate_proj),
        (v.conv_taps, hbm.conv_taps), (v.conv_state, hbm.conv_state),
        (v.decay_blocks, hbm.decay_blocks), (v.input_blocks, hbm.input_blocks),
        (v.decay_param, hbm.decay_param), (v.rec_state, hbm.rec_state),
    ):
        load(dst, (src, dst))
    load(v.out_proj, *[
        (hbm.out_proj.at[:, pl.ds(half * j, half)], v.out_proj.at[j]) for j in range(2)
    ])
    for dst, src in (
        (v.routing, hbm.routing), (v.route_weight, hbm.route_weight),
        (v.first_gain, hbm.first_gain),
    ):
        load(dst, (src, dst))
    starts = [
        (rel, core, pl.multiple_of(core * half + lax.rem(q + rel, 2) * quarter, quarter))
        for rel in range(2) for core in range(2)
    ]
    for dst, src in (v.dense_gate, hbm.dense_gate), (v.dense_up, hbm.dense_up):
        load(dst, *[
            (src.at[pl.ds(at, quarter), :], dst.at[rel, core]) for rel, core, at in starts
        ])
    for dst, src in (v.expert_gate, hbm.expert_gate), (v.expert_up, hbm.expert_up):
        load(dst, *[
            (src.at[:, pl.ds(at, quarter)], dst.at[rel, core]) for rel, core, at in starts
        ])
    for dst, src in (v.dense_down, hbm.dense_down), (v.expert_down, hbm.expert_down):
        load(dst, *[
            (
                src.at[:, pl.ds(128 * j, 128)],
                dst.at[j % 2, (j // 2) % 2, :, pl.ds(128 * (j // 4), 128)],
            )
            for j in range(ntp)
        ])
    for dst, src in (v.mix_weight, hbm.mix_weight), (v.second_gain, hbm.second_gain):
        load(dst, (src, dst))

    arrived(v.tokens, v.input_proj)
    inputs = dot(tok[...], v.input_proj[...]).astype(BF16)
    arrived(v.gate_proj)
    gated = dot(tok[...], v.gate_proj[...]).astype(BF16)
    arrived(v.conv_taps, v.conv_state, v.decay_blocks, v.input_blocks, v.decay_param, v.rec_state)
    taps = v.conv_taps[...].astype(F32)
    conv = inputs.astype(F32) * taps[3:4, :]
    for k in range(3):
        conv += v.conv_state[k].astype(F32) * taps[k : k + 1, :]
    convolved = conv.astype(BF16)
    recur_gate = jax.nn.sigmoid(dot(convolved, v.decay_blocks[0]))
    input_gate = jax.nn.sigmoid(dot(convolved, v.input_blocks[0]))
    param = v.decay_param[...]
    soft = jnp.maximum(-param, 0.0) + jnp.log1p(jnp.exp(-jnp.abs(param)))
    log_decay = -RATE_SCALE * recur_gate * soft
    state = jnp.exp(log_decay) * v.rec_state[...] + jnp.sqrt(
        one_less_exp(-2.0 * log_decay)
    ) * input_gate * convolved.astype(F32)
    g = gated.astype(F32)
    gelu = 0.5 * g * (1.0 + jnp.tanh(0.7978845608028654 * (g + 0.044715 * g * g * g)))
    mixed_rows = (state * gelu).astype(BF16)
    arrived(v.out_proj)
    v.pm_s[...] = dot(mixed_rows, v.out_proj[oc]).astype(BF16)

    pl.semaphore_wait(barrier, greeted)

    swap = send(v.pm_s, v.pm_r, "pm", 0, partner)
    v.pm_own[...] = dot(mixed_rows, v.out_proj[c])
    v.state[...] = state
    v.window[0] = v.conv_state[1]
    v.window[1] = v.conv_state[2]
    v.window[2] = inputs
    stores = [
        pltpu.make_async_copy(v.state, ns_o, sem["store"].at[0]),
        pltpu.make_async_copy(v.window, nc_o, sem["store"].at[1]),
    ]
    for copy in stores:
        copy.start()
    swap.wait_recv()
    v.zs[...] = (v.pm_own[...] + v.pm_r[...].astype(F32)).astype(BF16).reshape(
        nz, zrow, half
    )
    for k in far_first:
        send(v.zs.at[lax.rem(z + k, nz)], v.zr.at[z], "z", 0, zdev(k, c))

    arrived(v.routing, v.route_weight, v.first_gain)
    routes, route_weight = v.routing[...], v.route_weight[...]
    eids = lax.broadcasted_iota(jnp.int32, (ne, rows), 0)
    named = [routes[k : k + 1, :] == eids for k in range(TOPK)]
    either = jnp.where(named[0] | named[1], 1.0, 0.0)
    before = jnp.where(
        lax.broadcasted_iota(jnp.int32, (rows, rows), 0)
        < lax.broadcasted_iota(jnp.int32, (rows, rows), 1), 1.0, 0.0,
    )
    place = dot(either.astype(BF16), before.astype(BF16))
    slots = lax.broadcasted_iota(jnp.int32, (ne, cap, rows), 1).astype(F32)
    hit = (place[:, None, :] == slots) & (either[:, None, :] > 0.5)
    hot = jnp.where(hit, 1.0, 0.0)
    v.onehot[...] = hot.reshape(ny, group, rows).astype(BF16)
    weight = jnp.where(named[0], route_weight[0:1, :], 0.0)
    weight += jnp.where(named[1], route_weight[1:2, :], 0.0)
    weighted = (hot * weight[:, None, :]).reshape(ne * cap, rows).T
    upper = weighted.astype(BF16)
    v.wts[0:rows, :] = upper
    v.wts[rows:, :] = (weighted - upper.astype(F32)).astype(BF16)

    my_rows = pl.ds(pl.multiple_of(z * zrow, zrow), zrow)
    my_cols = pl.ds(pl.multiple_of(c * half, half), half)
    total = ALPHA * tok[my_rows, my_cols].astype(F32) + v.zs[z].astype(F32)
    whole(v.zr.at[pl.ds(0, nz - 1)], "z").wait_recv()
    for k in range(1, nz):
        total += v.zr[lax.rem(z - k + nz, nz)].astype(F32)

    row_mean = jnp.sum(total, axis=1, keepdims=True) / half
    row_m2 = jnp.sum(jnp.square(total - row_mean), axis=1, keepdims=True)
    v.st_s[0] = jnp.broadcast_to(row_mean, (zrow, 128))
    v.st_s[1] = jnp.broadcast_to(row_m2, (zrow, 128))
    send(v.st_s, v.st_r, "st", 0, partner).wait_recv()
    peer_mean, peer_m2 = v.st_r[0][:, 0:1], v.st_r[1][:, 0:1]
    mean = 0.5 * (row_mean + peer_mean)
    variance = (row_m2 + peer_m2 + jnp.square(row_mean - peer_mean) * (half / 2)) / d
    normed = (
        (total - mean) * lax.rsqrt(variance + NORM_EPS) * v.first_gain[:, my_cols]
    ).astype(BF16)
    first, second = normed[:, 0:quarter], normed[:, quarter:]
    even = q == 0
    nrm = v.nrm
    v.nother[...] = jnp.where(even, second, first)
    nrm[0, c, z] = jnp.where(even, first, second)

    for k in far_first:
        send(v.nother if k % 2 else nrm.at[0, c, z], nrm.at[0, c, z], "ag", 0, zdev(k, c))
    whole(nrm.at[0, c, pl.ds(0, nz - 1)], "ag").wait_recv()

    xin, ds = v.xin, v.ds
    offsets = [(dy, dx) for dy in range(ny) for dx in range(nx)]
    if ny == nx == 4:
        offsets = [
            (2, 2), (3, 2), (2, 3), (2, 1), (1, 2), (3, 1), (1, 3), (2, 0),
            (0, 2), (3, 3), (1, 1), (3, 0), (1, 0), (0, 3), (0, 1), (0, 0),
        ]
    direct = {ny - 1}
    beside = [f for f in range(ny) if f not in direct]

    def members(f):
        return list(enumerate(offsets))[f * nx : (f + 1) * nx]

    def dispatch(f, rel, out, name, at, done):
        for p, (dy, dx) in members(f):
            yy, e = lax.rem(y + dy, ny), edev(dy, dx)
            if dy not in done:
                done.add(dy)
                out[pl.ds(yy * nx, nx)] = dot(
                    v.onehot[yy], nrm[rel, c].reshape(rows, quarter)
                ).astype(BF16).reshape(nx, cap, quarter)
        for p, (dy, dx) in members(f):
            if dy or dx:
                e = edev(dy, dx)
                send(out.at[e], xin.at[rel, c, p], name, at, {"ep": e, "tp": tp})
            else:
                xin[rel, c, p] = out[ep]

    done = set()
    for f in range(ny):
        dispatch(f, 0, ds, "dx", f, done)

    first_z, last_z = pl.ds(0, hz), pl.ds(hz, hz)
    for part, k in (first_z, 1), (last_z, -1):
        send(nrm.at[0, c, part], nrm.at[1, c, part], "nz", 0, zdev(k, c))
    send(nrm.at[0, c], nrm.at[0, c], "np", 0, partner)

    per = min(2, ny)
    flight = {}

    def halves(src, dst, count, name, at):
        for part, k in (pl.ds(0, count // 2), 1), (pl.ds(count // 2, count // 2), -1):
            send(src.at[part], dst.at[part], name, at, zdev(k, c))
        return whole(dst, name, at)

    def normed_beside(_):
        whole(nrm.at[1, c], "nz").wait_recv()
        send(nrm.at[1, c], nrm.at[1, c], "np", 0, partner)
        done = set()
        for f in sorted(direct):
            dispatch(f, 1, v.ds2, "d2", f, done)

    def arrive(f):
        count = len([p for p, at in members(f) if at != (0, 0)])
        whole(xin.at[0, c, pl.ds(f * nx, count)], "dx", f).wait_recv()
        row = pl.ds(f * nx, nx)
        if f not in direct:
            flight["z", f] = halves(xin.at[0, c, row], xin.at[1, c, row], nx, "xz", f)
        flight["own", f] = send(xin.at[0, c, row], xin.at[0, c, row], "xp", 2 * f, partner)

    def hand_over(f):
        if f not in direct:
            flight["z", f].wait_recv()
        else:
            count = len([p for p, at in members(f) if at != (0, 0)])
            whole(xin.at[1, c, pl.ds(f * nx, count)], "d2", f).wait_recv()
        row = pl.ds(f * nx, nx)
        flight["other", f] = send(xin.at[1, c, row], xin.at[1, c, row], "xp", 2 * f + 1, partner)

    def gate_up(k, rel):
        pieces = [
            xin[rel, core, pl.ds(k * per * nx, per * nx)].reshape(per * group, quarter)
            for core in range(2)
        ]
        return [
            dot_nt(pieces[0], weights[rel, 0]) + dot_nt(pieces[1], weights[rel, 1])
            for weights in (v.expert_gate, v.expert_up)
        ]

    def compute_own(k):
        if k == 0:
            arrived(v.expert_gate, v.expert_up)
        for f in range(k * per, (k + 1) * per):
            flight["own", f].wait_recv()
        v.gate[k], v.up[k] = gate_up(k, 0)

    def compute_other(k):
        for f in range(k * per, (k + 1) * per):
            flight["other", f].wait_recv()
        gate, up = gate_up(k, 1)
        v.hidden[k] = (jax.nn.silu(v.gate[k] + gate) * (v.up[k] + up)).astype(BF16)

    def down(k):
        fine = range(k * per, (k + 1) * per)
        if k == 0:
            arrived(v.expert_down)
        hidden = v.hidden[k]
        for j, par in enumerate((1 - q, q)):
            product = dot(hidden, v.expert_down[oc, par]).astype(BF16)
            for f in fine:
                at = (f - k * per) * group
                v.ps[f, j] = product[at : at + group]
                flight["sum", f, j] = send(
                    v.ps.at[f, j], v.pr.at[f, j], "po", 2 * f + j, partner
                )
        for j, par in enumerate((1 - q, q)):
            product = dot(hidden, v.expert_down[c, par])
            for f in fine:
                at = (f - k * per) * group
                v.po[f, j] = product[at : at + group]

    def pair_sum(f):
        flight["sum", f, 0].wait_recv()
        v.bs[f] = (v.po[f, 0] + v.pr[f, 0].astype(F32)).astype(BF16)
        flight["beside", f] = halves(v.bs.at[f], v.br.at[f], group, "bz", f)

    def go_home(f):
        flight["sum", f, 1].wait_recv()
        flight["beside", f].wait_recv()
        v.rs[pl.ds(f * nx, nx)] = (
            v.po[f, 1] + v.pr[f, 1].astype(F32) + v.br[f].astype(F32)
        ).astype(BF16).reshape(nx, cap, quarter)
        for p, (dy, dx) in members(f):
            if dy or dx:
                home = {"ep": edev(-dy, -dx), "tp": tp}
                send(v.rs.at[p], v.ret.at[ep], "rt", 0, home)
            else:
                v.ret[ep] = v.rs[p]

    def dense_start(_):
        arrived(v.dense_gate, v.dense_up, v.dense_down, v.mix_weight)
        whole(nrm.at[:, c], "np").wait_recv()
        gate = up = mixing = None
        v.mixf[...] = v.mix_weight[...].astype(F32)
        for rel, core, _ in starts:
            piece = nrm[rel, core].reshape(rows, quarter)
            more = dot(piece, v.dense_gate[rel, core])
            gate = more if gate is None else gate + more
            more = dot(piece, v.dense_up[rel, core])
            up = more if up is None else up + more
            for j in range(quarter // 128):
                at = (core * 2 + lax.rem(q + rel, 2)) * (quarter // 128) + j
                more = piece[:, 128 * j : 128 * (j + 1)].astype(F32) * v.mixf[pl.ds(at, 1), :]
                mixing = more if mixing is None else mixing + more
        hidden = (jax.nn.silu(gate) * up).astype(BF16)
        for j, par in enumerate((1 - q, q)):
            v.dps[j] = dot(hidden, v.dense_down[oc, par]).astype(BF16)
        flight["dense"] = send(v.dps, v.dpr, "dp", 0, partner)
        for j, par in enumerate((1 - q, q)):
            v.dpo[j] = dot(hidden, v.dense_down[c, par])
        v.mix[...] = jnp.broadcast_to(
            jax.nn.sigmoid(jnp.sum(mixing, axis=1, keepdims=True)), (rows, 128)
        )

    def dense_pair(_):
        flight["dense"].wait_recv()
        v.dbs[...] = (v.dpo[0] + v.dpr[0].astype(F32)).astype(BF16)
        flight["dense_beside"] = halves(v.dbs, v.dbr, rows, "db", 0)

    def dense_end(_):
        flight["dense_beside"].wait_recv()
        v.dacc[...] = v.mix[:, 0:1] * (
            v.dpo[1] + v.dpr[1].astype(F32) + v.dbr[...].astype(F32)
        )

    plan = [
        (normed_beside, 0), (arrive, 0), (arrive, 1), (arrive, 2), (dense_start, 0), (arrive, 3),
        (hand_over, 0), (compute_own, 0), (hand_over, 1), (hand_over, 3), (compute_own, 1),
        (compute_other, 0), (hand_over, 2), (down, 0), (pair_sum, 0), (pair_sum, 1),
        (compute_other, 1), (down, 1), (pair_sum, 2), (pair_sum, 3), (dense_pair, 0), (go_home, 0),
        (go_home, 1), (go_home, 2), (go_home, 3), (dense_end, 0),
    ]
    for step, which in plan:
        if which < (ny // per if step in (compute_own, compute_other, down) else ny):
            step(which)

    whole(v.ret.at[pl.ds(0, ne - 1)], "rt").wait_recv()
    both = dot(v.wts[...], v.ret[...].reshape(ne * cap, quarter))
    fin = v.dacc[...] + both[0:rows] + both[rows:]
    for k in range(hz):
        v.fs[k] = fin[:, 128 * k : 128 * (k + 1)].astype(BF16)
    zh = lax.div(z, 2)
    for k in sorted(range(1, hz), key=lambda k: -min(k, hz - k)):
        send(v.fs.at[lax.rem(zh + k, hz)], v.fr.at[zh], "f", 0, zdev(2 * k, c))
    place_of = lax.rem(tp, nz)
    column = pl.ds(pl.multiple_of(lax.rem(place_of, hz) * 128, 128), 128)
    own = nrm[lax.rem(lax.div(place_of, hz) + q, 2), lax.div(tp, nz), :, :, column]
    combined = ALPHA * own.reshape(rows, 128).astype(F32) + v.fs[zh].astype(F32)
    if hz > 1:
        whole(v.fr.at[pl.ds(0, hz - 1)], "f").wait_recv()
    for k in range(1, hz):
        combined += v.fr[lax.rem(zh - k + hz, hz)].astype(F32)

    arrived(v.second_gain)
    turned = combined.T
    block_mean = jnp.sum(turned, axis=0, keepdims=True) / 128
    block_m2 = jnp.sum(jnp.square(turned - block_mean), axis=0, keepdims=True)
    v.ss[...] = jnp.concatenate([block_mean, block_m2, jnp.zeros((6, rows), F32)], axis=0)
    peers = [
        (k, core, 2 * k + j)
        for k in far_first + [0] for j, core in enumerate((c, oc)) if k or j
    ]
    for k, core, i in peers:
        send(v.ss, v.sr.at[i], "s", 0, zdev(k, core))
    whole(v.sr.at[pl.ds(0, ntp - 1)], "s").wait_recv()
    stats = [v.ss[...]] + [v.sr[i] for _, _, i in peers]
    mean = sum(s[0:1] for s in stats) / ntp
    m2 = sum(s[1:2] + 128 * jnp.square(s[0:1] - mean) for s in stats)
    scaled = ((turned - mean) * lax.rsqrt(m2 / d + NORM_EPS)).T
    v.out[...] = (scaled * v.second_gain[...]).astype(BF16)
    stores.append(pltpu.make_async_copy(v.out, lo_o, sem["store"].at[2]))
    stores[-1].start()
    for name, ref in (
        ("pm", v.pm_s), ("z", v.zs.at[pl.ds(0, nz - 1)]), ("st", v.st_s),
        ("ag", nrm.at[0, c, pl.ds(0, nz - 1)]), ("np", nrm.at[:, c]), ("nz", nrm.at[0, c]),
        ("dx", ds.at[pl.ds(0, ne - 1)]), ("xz", xin.at[0, c, pl.ds(0, len(beside) * nx)]),
        ("d2", xin.at[0, c, pl.ds(0, len(direct) * nx - 1)]), ("xp", xin.at[:, c]),
        ("po", v.ps), ("bz", v.bs), ("rt", v.rs.at[pl.ds(0, ne - 1)]), ("dp", v.dps),
        ("db", v.dbs), ("f", v.fs.at[pl.ds(0, hz - 1)]), ("s", v.sr.at[pl.ds(0, ntp - 1)]),
    ):
        if 0 not in ref.shape:
            whole(ref, name).wait_send()
    for copy in stores:
        copy.wait()


def hand_out(*refs):
    arrays, sem = refs[:9], refs[9]
    moves = [
        [pltpu.make_async_copy(arrays[i], arrays[6 + i], sem.at[i]) for i in range(3)],
        [pltpu.make_async_copy(arrays[6 + i], arrays[3 + i], sem.at[3 + i]) for i in range(3)],
    ]
    for copy in moves[0]:
        copy.start()
    for into, out in zip(*moves):
        into.wait()
        out.start()
    for copy in moves[1]:
        copy.wait()


def on_device(nz, ny, nx, *arrays):
    args = Args(*arrays)
    rows, d = args.tokens.shape
    ff = args.expert_gate.shape[2]
    args = args._replace(
        conv_state=args.conv_state.transpose(1, 0, 2),
        decay_param=args.decay_param.reshape(1, -1),
        first_gain=args.first_gain.reshape(1, -1),
        second_gain=args.second_gain.reshape(1, -1),
        expert_gate=args.expert_gate[0].T,
        expert_up=args.expert_up[0].T,
        expert_down=args.expert_down[0],
        routing=args.routing.T,
        route_weight=args.route_weight.T,
        mix_weight=args.mix_weight.reshape(-1, 128),
    )

    half, quarter = d // 2, d // 4
    ne, ntp, hz = ny * nx, 2 * nz, nz // 2
    cap = max(2, 2 * rows * TOPK // ne)
    group, zrow = nx * cap, rows // nz
    rows_at_once = min(2, ny) * group
    ng = ne * cap // rows_at_once
    scratch = {name: (a.shape, a.dtype) for name, a in args._asdict().items()}
    scratch.update(
        out_proj=((2, rows, half), BF16),
        expert_gate=((2, 2, ff, quarter), BF16), expert_up=((2, 2, ff, quarter), BF16),
        expert_down=((2, 2, ff, quarter), BF16),
        dense_gate=((2, 2, quarter, 128), BF16), dense_up=((2, 2, quarter, 128), BF16),
        dense_down=((2, 2, 128, quarter), BF16),
        pm_s=((rows, half), BF16), pm_r=((rows, half), BF16), pm_own=((rows, half), F32),
        state=((rows, 128), F32), window=((3, rows, 128), BF16), out=((rows, 128), BF16),
        zs=((nz, zrow, half), BF16), zr=((nz, zrow, half), BF16),
        st_s=((2, zrow, 128), F32), st_r=((2, zrow, 128), F32),
        nrm=((2, 2, nz, zrow, quarter), BF16), nother=((zrow, quarter), BF16),
        onehot=((ny, group, rows), BF16), wts=((2 * rows, ne * cap), BF16),
        ds=((ne, cap, quarter), BF16), ds2=((ne, cap, quarter), BF16),
        hidden=((ng, rows_at_once, ff), BF16), xin=((2, 2, ne, cap, quarter), BF16),
        ps=((ny, 2, group, quarter), BF16), pr=((ny, 2, group, quarter), BF16),
        po=((ny, 2, group, quarter), F32), gate=((ng, rows_at_once, ff), F32),
        up=((ng, rows_at_once, ff), F32),
        bs=((ny, group, quarter), BF16), br=((ny, group, quarter), BF16),
        rs=((ne, cap, quarter), BF16), ret=((ne, cap, quarter), BF16),
        mixf=((d // 128, 128), F32), mix=((rows, 128), F32),
        dps=((2, rows, quarter), BF16), dpr=((2, rows, quarter), BF16),
        dpo=((2, rows, quarter), F32), dbs=((rows, quarter), BF16), dbr=((rows, quarter), BF16),
        dacc=((rows, quarter), F32),
        fs=((hz, rows, 128), BF16), fr=((hz, rows, 128), BF16),
        ss=((8, rows), F32), sr=((ntp, 8, rows), F32),
    )
    pairs = dict(
        pm=1, z=1, st=1, ag=1, np=1, nz=1, dx=ny, d2=ny, xz=ny, xp=2 * ny, po=2 * ny, bz=ny, rt=1, dp=1,
        db=1, f=1, s=1,
    )
    sems = {"load": len(args), "store": 3}
    for name, n in pairs.items():
        sems[name + "_s"], sems[name + "_r"] = 1, n
    anywhere = pl.BlockSpec(memory_space=pl.ANY)
    outs = (
        jax.ShapeDtypeStruct((rows, 128), BF16),
        jax.ShapeDtypeStruct((rows, 128), F32),
        jax.ShapeDtypeStruct((3, rows, 128), BF16),
    )
    labels = tuple(scratch), tuple(sems)
    results = pl.pallas_call(
        functools.partial(kernel, nz, ny, nx, cap, labels),
        name="decode_step",
        out_shape=outs,
        in_specs=[anywhere] * len(args),
        out_specs=(anywhere,) * 3,
        scratch_shapes=[pltpu.VMEM(*s) for s in scratch.values()]
        + [pltpu.SemaphoreType.DMA((n,)) for n in sems.values()],
        compiler_params=pltpu.CompilerParams(collective_id=0, has_side_effects=True),
    )(*args)
    layer_out, new_state, new_conv = pl.pallas_call(
        hand_out,
        name="hand_out",
        out_shape=outs,
        in_specs=[anywhere] * 3,
        out_specs=(anywhere,) * 3,
        scratch_shapes=[pltpu.VMEM(s.shape, s.dtype) for s in outs]
        + [pltpu.SemaphoreType.DMA((6,))],
    )(*results)
    return layer_out, new_state, new_conv.transpose(1, 0, 2)


def solution(mesh):
    ep, tp = mesh.shape["ep"], mesh.shape["tp"]
    nx = {16: 4, 4: 2, 2: 2}[ep]
    return jax.shard_map(
        functools.partial(on_device, tp // 2, ep // nx, nx),
        mesh=mesh,
        in_specs=(
            P("ep", None), P("ep", None, "tp"), P("ep", "tp"), P(None, "tp"), P(None, "tp"),
            P(None, "tp"), P("tp", None, None), P("tp", None, None), P("tp"), P("tp", None), P(),
            P("ep", None, "tp"), P("ep", None, "tp"), P("ep", "tp", None), P("ep", None),
            P("ep", None), P(None, "tp"), P(None, "tp"), P("tp", None), P(), P("tp"),
        ),
        out_specs=(P("ep", "tp"), P("ep", "tp"), P("ep", None, "tp")),
        check_vma=False,
    )
```

```python
import functools
from types import SimpleNamespace
from typing import Any, NamedTuple

import jax
import jax.numpy as jnp
from jax import lax
from jax.experimental import pallas as pl
from jax.experimental.pallas import tpu as pltpu
from jax.sharding import PartitionSpec as P

MESH = pl.DeviceIdType.MESH
ALPHA = 8.0**0.25
RATE_SCALE = 8.0
NORM_EPS = 1e-05
TOPK = 2
F32 = jnp.float32
BF16 = jnp.bfloat16


class Args(NamedTuple):
    tokens: Any
    conv_state: Any
    rec_state: Any
    gate_proj: Any
    input_proj: Any
    conv_taps: Any
    decay_blocks: Any
    input_blocks: Any
    decay_param: Any
    out_proj: Any
    first_gain: Any
    expert_gate: Any
    expert_up: Any
    expert_down: Any
    routing: Any
    route_weight: Any
    dense_gate: Any
    dense_up: Any
    dense_down: Any
    mix_weight: Any
    second_gain: Any


def dot(a, b):
    return jnp.dot(a, b, preferred_element_type=F32)


def dot_nt(a, b):
    return lax.dot_general(a, b, (((1,), (1,)), ((), ())), preferred_element_type=F32)


def one_less_exp(u):
    series = 1.0 - u * (1.0 / 8.0)
    for k in (7, 6, 5, 4, 3, 2):
        series = 1.0 - u * (1.0 / k) * series
    return jnp.where(u < 0.5, u * series, 1.0 - jnp.exp(-u))


def kernel(nz, ny, nx, cap, names, *refs):
    hbm = Args(*refs[: len(Args._fields)])
    refs = refs[len(hbm) :]
    lo_o, ns_o, nc_o = refs[:3]
    v = SimpleNamespace(**dict(zip(names[0], refs[3:])))
    sem = dict(zip(names[1], refs[3 + len(names[0]) :]))

    tok = v.tokens
    ne, ntp = ny * nx, 2 * nz
    rows, d = tok.shape
    half, quarter = d // 2, d // 4
    zrow, hz, group = rows // nz, nz // 2, nx * cap
    ep, tp = lax.axis_index("ep"), lax.axis_index("tp")
    z, c = lax.div(tp, 2), lax.rem(tp, 2)
    oc, q = 1 - c, lax.rem(z, 2)
    y, x = lax.div(ep, nx), lax.rem(ep, nx)
    partner = {"ep": ep, "tp": 2 * z + oc}

    def zdev(k, core):
        return {"ep": ep, "tp": 2 * lax.rem(z + k + nz, nz) + core}

    def edev(dy, dx):
        return lax.rem(y + dy + ny, ny) * nx + lax.rem(x + dx + nx, nx)

    def send(src, dst, name, i, dev):
        copy = pltpu.make_async_remote_copy(
            src_ref=src, dst_ref=dst,
            send_sem=sem[name + "_s"].at[0], recv_sem=sem[name + "_r"].at[i],
            device_id=dev, device_id_type=MESH,
        )
        copy.start()
        return copy

    def whole(ref, name, i=0):
        return pltpu.make_async_remote_copy(
            src_ref=ref, dst_ref=ref,
            send_sem=sem[name + "_s"].at[0], recv_sem=sem[name + "_r"].at[i],
            device_id=partner, device_id_type=MESH,
        )

    loads = {}

    def load(dst, *pieces):
        at = sem["load"].at[len(loads)]
        loads[id(dst)] = pltpu.make_async_copy(dst, dst, at)
        for src, part in pieces:
            pltpu.make_async_copy(src, part, at).start()

    def arrived(*wanted):
        for dst in wanted:
            loads[id(dst)].wait()

    for dst, src in (
        (v.tokens, hbm.tokens), (v.input_proj, hbm.input_proj), (v.gate_proj, hbm.gate_proj),
    ):
        load(dst, (src, dst))

    far_first = sorted(range(1, nz), key=lambda k: -min(k, nz - k))

    barrier = pltpu.get_barrier_semaphore()
    greeted = 0
    for k in far_first + [0]:
        for j, core in enumerate((c, oc)):
            if k or j:
                pl.semaphore_signal(barrier, inc=1, device_id=zdev(k, core), device_id_type=MESH)
                greeted += 1
    for dy in range(ny):
        for dx in range(nx):
            if dy or dx:
                pl.semaphore_signal(
                    barrier, inc=1, device_id={"ep": edev(dy, dx), "tp": tp}, device_id_type=MESH
                )
                greeted += 1

    for dst, src in (
        (v.conv_taps, hbm.conv_taps), (v.conv_state, hbm.conv_state),
        (v.decay_blocks, hbm.decay_blocks), (v.input_blocks, hbm.input_blocks),
        (v.decay_param, hbm.decay_param), (v.rec_state, hbm.rec_state),
    ):
        load(dst, (src, dst))
    load(v.out_proj, *[
        (hbm.out_proj.at[:, pl.ds(half * j, half)], v.out_proj.at[j]) for j in range(2)
    ])
    for dst, src in (
        (v.routing, hbm.routing), (v.route_weight, hbm.route_weight),
        (v.first_gain, hbm.first_gain),
    ):
        load(dst, (src, dst))
    starts = [
        (rel, core, pl.multiple_of(core * half + lax.rem(q + rel, 2) * quarter, quarter))
        for rel in range(2) for core in range(2)
    ]
    for dst, src in (v.dense_gate, hbm.dense_gate), (v.dense_up, hbm.dense_up):
        load(dst, *[
            (src.at[pl.ds(at, quarter), :], dst.at[rel, core]) for rel, core, at in starts
        ])
    for dst, src in (v.expert_gate, hbm.expert_gate), (v.expert_up, hbm.expert_up):
        load(dst, *[
            (src.at[:, pl.ds(at, quarter)], dst.at[rel, core]) for rel, core, at in starts
        ])
    for dst, src in (v.dense_down, hbm.dense_down), (v.expert_down, hbm.expert_down):
        load(dst, *[
            (
                src.at[:, pl.ds(128 * j, 128)],
                dst.at[j % 2, (j // 2) % 2, :, pl.ds(128 * (j // 4), 128)],
            )
            for j in range(ntp)
        ])
    for dst, src in (v.mix_weight, hbm.mix_weight), (v.second_gain, hbm.second_gain):
        load(dst, (src, dst))

    arrived(v.tokens, v.input_proj)
    inputs = dot(tok[...], v.input_proj[...]).astype(BF16)
    arrived(v.gate_proj)
    gated = dot(tok[...], v.gate_proj[...]).astype(BF16)
    arrived(v.conv_taps, v.conv_state, v.decay_blocks, v.input_blocks, v.decay_param, v.rec_state)
    taps = v.conv_taps[...].astype(F32)
    conv = inputs.astype(F32) * taps[3:4, :]
    for k in range(3):
        conv += v.conv_state[k].astype(F32) * taps[k : k + 1, :]
    convolved = conv.astype(BF16)
    recur_gate = jax.nn.sigmoid(dot(convolved, v.decay_blocks[0]))
    input_gate = jax.nn.sigmoid(dot(convolved, v.input_blocks[0]))
    param = v.decay_param[...]
    soft = jnp.maximum(-param, 0.0) + jnp.log1p(jnp.exp(-jnp.abs(param)))
    log_decay = -RATE_SCALE * recur_gate * soft
    state = jnp.exp(log_decay) * v.rec_state[...] + jnp.sqrt(
        one_less_exp(-2.0 * log_decay)
    ) * input_gate * convolved.astype(F32)
    g = gated.astype(F32)
    gelu = 0.5 * g * (1.0 + jnp.tanh(0.7978845608028654 * (g + 0.044715 * g * g * g)))
    mixed_rows = (state * gelu).astype(BF16)
    arrived(v.out_proj)
    v.pm_s[...] = dot(mixed_rows, v.out_proj[oc]).astype(BF16)

    pl.semaphore_wait(barrier, greeted)

    swap = send(v.pm_s, v.pm_r, "pm", 0, partner)
    v.pm_own[...] = dot(mixed_rows, v.out_proj[c])
    v.state[...] = state
    v.window[0] = v.conv_state[1]
    v.window[1] = v.conv_state[2]
    v.window[2] = inputs
    stores = [
        pltpu.make_async_copy(v.state, ns_o, sem["store"].at[0]),
        pltpu.make_async_copy(v.window, nc_o, sem["store"].at[1]),
    ]
    for copy in stores:
        copy.start()
    swap.wait_recv()
    v.zs[...] = (v.pm_own[...] + v.pm_r[...].astype(F32)).astype(BF16).reshape(
        nz, zrow, half
    )
    for k in far_first:
        send(v.zs.at[lax.rem(z + k, nz)], v.zr.at[z], "z", 0, zdev(k, c))

    arrived(v.routing, v.route_weight, v.first_gain)
    routes, route_weight = v.routing[...], v.route_weight[...]
    eids = lax.broadcasted_iota(jnp.int32, (ne, rows), 0)
    named = [routes[k : k + 1, :] == eids for k in range(TOPK)]
    either = jnp.where(named[0] | named[1], 1.0, 0.0)
    before = jnp.where(
        lax.broadcasted_iota(jnp.int32, (rows, rows), 0)
        < lax.broadcasted_iota(jnp.int32, (rows, rows), 1), 1.0, 0.0,
    )
    place = dot(either.astype(BF16), before.astype(BF16))
    slots = lax.broadcasted_iota(jnp.int32, (ne, cap, rows), 1).astype(F32)
    hit = (place[:, None, :] == slots) & (either[:, None, :] > 0.5)
    hot = jnp.where(hit, 1.0, 0.0)
    v.onehot[...] = hot.reshape(ny, group, rows).astype(BF16)
    weight = jnp.where(named[0], route_weight[0:1, :], 0.0)
    weight += jnp.where(named[1], route_weight[1:2, :], 0.0)
    weighted = (hot * weight[:, None, :]).reshape(ne * cap, rows).T
    upper = weighted.astype(BF16)
    v.wts[0:rows, :] = upper
    v.wts[rows:, :] = (weighted - upper.astype(F32)).astype(BF16)

    my_rows = pl.ds(pl.multiple_of(z * zrow, zrow), zrow)
    my_cols = pl.ds(pl.multiple_of(c * half, half), half)
    total = ALPHA * tok[my_rows, my_cols].astype(F32) + v.zs[z].astype(F32)
    whole(v.zr.at[pl.ds(0, nz - 1)], "z").wait_recv()
    for k in range(1, nz):
        total += v.zr[lax.rem(z - k + nz, nz)].astype(F32)

    row_mean = jnp.sum(total, axis=1, keepdims=True) / half
    row_m2 = jnp.sum(jnp.square(total - row_mean), axis=1, keepdims=True)
    v.st_s[0] = jnp.broadcast_to(row_mean, (zrow, 128))
    v.st_s[1] = jnp.broadcast_to(row_m2, (zrow, 128))
    send(v.st_s, v.st_r, "st", 0, partner).wait_recv()
    peer_mean, peer_m2 = v.st_r[0][:, 0:1], v.st_r[1][:, 0:1]
    mean = 0.5 * (row_mean + peer_mean)
    variance = (row_m2 + peer_m2 + jnp.square(row_mean - peer_mean) * (half / 2)) / d
    normed = (
        (total - mean) * lax.rsqrt(variance + NORM_EPS) * v.first_gain[:, my_cols]
    ).astype(BF16)
    first, second = normed[:, 0:quarter], normed[:, quarter:]
    even = q == 0
    nrm = v.nrm
    v.nother[...] = jnp.where(even, second, first)
    nrm[0, c, z] = jnp.where(even, first, second)

    for k in far_first:
        send(v.nother if k % 2 else nrm.at[0, c, z], nrm.at[0, c, z], "ag", 0, zdev(k, c))
    whole(nrm.at[0, c, pl.ds(0, nz - 1)], "ag").wait_recv()

    xin, ds = v.xin, v.ds
    offsets = [(dy, dx) for dy in range(ny) for dx in range(nx)]
    if ny == nx == 4:
        offsets = [
            (2, 2), (3, 2), (2, 3), (2, 1), (1, 2), (3, 1), (1, 3), (2, 0),
            (0, 2), (3, 3), (1, 1), (3, 0), (1, 0), (0, 3), (0, 1), (0, 0),
        ]
    direct = {ny - 1}
    beside = [f for f in range(ny) if f not in direct]

    def members(f):
        return list(enumerate(offsets))[f * nx : (f + 1) * nx]

    def dispatch(f, rel, out, name, at, done):
        for p, (dy, dx) in members(f):
            yy, e = lax.rem(y + dy, ny), edev(dy, dx)
            if dy not in done:
                done.add(dy)
                out[pl.ds(yy * nx, nx)] = dot(
                    v.onehot[yy], nrm[rel, c].reshape(rows, quarter)
                ).astype(BF16).reshape(nx, cap, quarter)
        for p, (dy, dx) in members(f):
            if dy or dx:
                e = edev(dy, dx)
                send(out.at[e], xin.at[rel, c, p], name, at, {"ep": e, "tp": tp})
            else:
                xin[rel, c, p] = out[ep]

    done = set()
    for f in range(ny):
        dispatch(f, 0, ds, "dx", f, done)

    first_z, last_z = pl.ds(0, hz), pl.ds(hz, hz)
    for part, k in (first_z, 1), (last_z, -1):
        send(nrm.at[0, c, part], nrm.at[1, c, part], "nz", 0, zdev(k, c))
    send(nrm.at[0, c], nrm.at[0, c], "np", 0, partner)

    per = min(2, ny)
    flight = {}

    def halves(src, dst, count, name, at):
        for part, k in (pl.ds(0, count // 2), 1), (pl.ds(count // 2, count // 2), -1):
            send(src.at[part], dst.at[part], name, at, zdev(k, c))
        return whole(dst, name, at)

    def normed_beside(_):
        whole(nrm.at[1, c], "nz").wait_recv()
        send(nrm.at[1, c], nrm.at[1, c], "np", 0, partner)
        done = set()
        for f in sorted(direct):
            dispatch(f, 1, v.ds2, "d2", 0, done)

    def arrive(f):
        count = len([p for p, at in members(f) if at != (0, 0)])
        whole(xin.at[0, c, pl.ds(f * nx, count)], "dx", f).wait_recv()
        row = pl.ds(f * nx, nx)
        if f not in direct:
            flight["z", f] = halves(xin.at[0, c, row], xin.at[1, c, row], nx, "xz", f)
        flight["own", f] = send(xin.at[0, c, row], xin.at[0, c, row], "xp", 2 * f, partner)

    def hand_over(f):
        if f not in direct:
            flight["z", f].wait_recv()
        else:
            count = len([p for p, at in members(f) if at != (0, 0)])
            whole(xin.at[1, c, pl.ds(f * nx, count)], "d2").wait_recv()
        row = pl.ds(f * nx, nx)
        flight["other", f] = send(xin.at[1, c, row], xin.at[1, c, row], "xp", 2 * f + 1, partner)

    def gate_up(k, rel):
        pieces = [
            xin[rel, core, pl.ds(k * per * nx, per * nx)].reshape(per * group, quarter)
            for core in range(2)
        ]
        return [
            dot_nt(pieces[0], weights[rel, 0]) + dot_nt(pieces[1], weights[rel, 1])
            for weights in (v.expert_gate, v.expert_up)
        ]

    def compute_own(k):
        if k == 0:
            arrived(v.expert_gate, v.expert_up)
        for f in range(k * per, (k + 1) * per):
            flight["own", f].wait_recv()
        v.gate[k], v.up[k] = gate_up(k, 0)

    def compute_other(k):
        for f in range(k * per, (k + 1) * per):
            flight["other", f].wait_recv()
        gate, up = gate_up(k, 1)
        v.hidden[k] = (jax.nn.silu(v.gate[k] + gate) * (v.up[k] + up)).astype(BF16)

    def down(k):
        fine = range(k * per, (k + 1) * per)
        if k == 0:
            arrived(v.expert_down)
        hidden = v.hidden[k]
        for j, par in enumerate((1 - q, q)):
            product = dot(hidden, v.expert_down[oc, par]).astype(BF16)
            for f in fine:
                at = (f - k * per) * group
                v.ps[f, j] = product[at : at + group]
                flight["sum", f, j] = send(
                    v.ps.at[f, j], v.pr.at[f, j], "po", 2 * f + j, partner
                )
        for j, par in enumerate((1 - q, q)):
            product = dot(hidden, v.expert_down[c, par])
            for f in fine:
                at = (f - k * per) * group
                v.po[f, j] = product[at : at + group]

    def pair_sum(f):
        flight["sum", f, 0].wait_recv()
        v.bs[f] = (v.po[f, 0] + v.pr[f, 0].astype(F32)).astype(BF16)
        flight["beside", f] = halves(v.bs.at[f], v.br.at[f], group, "bz", f)

    def go_home(f):
        flight["sum", f, 1].wait_recv()
        flight["beside", f].wait_recv()
        v.rs[pl.ds(f * nx, nx)] = (
            v.po[f, 1] + v.pr[f, 1].astype(F32) + v.br[f].astype(F32)
        ).astype(BF16).reshape(nx, cap, quarter)
        for p, (dy, dx) in members(f):
            if dy or dx:
                home = {"ep": edev(-dy, -dx), "tp": tp}
                send(v.rs.at[p], v.ret.at[ep], "rt", 0, home)
            else:
                v.ret[ep] = v.rs[p]

    def dense_start(_):
        arrived(v.dense_gate, v.dense_up, v.dense_down, v.mix_weight)
        whole(nrm.at[:, c], "np").wait_recv()
        gate = up = mixing = None
        v.mixf[...] = v.mix_weight[...].astype(F32)
        for rel, core, _ in starts:
            piece = nrm[rel, core].reshape(rows, quarter)
            more = dot(piece, v.dense_gate[rel, core])
            gate = more if gate is None else gate + more
            more = dot(piece, v.dense_up[rel, core])
            up = more if up is None else up + more
            for j in range(quarter // 128):
                at = (core * 2 + lax.rem(q + rel, 2)) * (quarter // 128) + j
                more = piece[:, 128 * j : 128 * (j + 1)].astype(F32) * v.mixf[pl.ds(at, 1), :]
                mixing = more if mixing is None else mixing + more
        hidden = (jax.nn.silu(gate) * up).astype(BF16)
        for j, par in enumerate((1 - q, q)):
            v.dps[j] = dot(hidden, v.dense_down[oc, par]).astype(BF16)
        flight["dense"] = send(v.dps, v.dpr, "dp", 0, partner)
        for j, par in enumerate((1 - q, q)):
            v.dpo[j] = dot(hidden, v.dense_down[c, par])
        v.mix[...] = jnp.broadcast_to(
            jax.nn.sigmoid(jnp.sum(mixing, axis=1, keepdims=True)), (rows, 128)
        )

    def dense_pair(_):
        flight["dense"].wait_recv()
        v.dbs[...] = (v.dpo[0] + v.dpr[0].astype(F32)).astype(BF16)
        flight["dense_beside"] = halves(v.dbs, v.dbr, rows, "db", 0)

    def dense_end(_):
        flight["dense_beside"].wait_recv()
        v.dacc[...] = v.mix[:, 0:1] * (
            v.dpo[1] + v.dpr[1].astype(F32) + v.dbr[...].astype(F32)
        )

    plan = [
        (normed_beside, 0), (arrive, 0), (arrive, 1), (arrive, 2), (dense_start, 0), (arrive, 3),
        (hand_over, 0), (compute_own, 0), (hand_over, 1), (hand_over, 3), (compute_own, 1),
        (compute_other, 0), (hand_over, 2), (down, 0), (pair_sum, 0), (pair_sum, 1),
        (compute_other, 1), (down, 1), (pair_sum, 2), (pair_sum, 3), (dense_pair, 0), (go_home, 0),
        (go_home, 1), (go_home, 2), (go_home, 3), (dense_end, 0),
    ]
    for step, which in plan:
        if which < (ny // per if step in (compute_own, compute_other, down) else ny):
            step(which)

    whole(v.ret.at[pl.ds(0, ne - 1)], "rt").wait_recv()
    both = dot(v.wts[...], v.ret[...].reshape(ne * cap, quarter))
    fin = v.dacc[...] + both[0:rows] + both[rows:]
    for k in range(hz):
        v.fs[k] = fin[:, 128 * k : 128 * (k + 1)].astype(BF16)
    zh = lax.div(z, 2)
    for k in sorted(range(1, hz), key=lambda k: -min(k, hz - k)):
        send(v.fs.at[lax.rem(zh + k, hz)], v.fr.at[zh], "f", 0, zdev(2 * k, c))
    place_of = lax.rem(tp, nz)
    column = pl.ds(pl.multiple_of(lax.rem(place_of, hz) * 128, 128), 128)
    own = nrm[lax.rem(lax.div(place_of, hz) + q, 2), lax.div(tp, nz), :, :, column]
    combined = ALPHA * own.reshape(rows, 128).astype(F32) + v.fs[zh].astype(F32)
    if hz > 1:
        whole(v.fr.at[pl.ds(0, hz - 1)], "f").wait_recv()
    for k in range(1, hz):
        combined += v.fr[lax.rem(zh - k + hz, hz)].astype(F32)

    arrived(v.second_gain)
    turned = combined.T
    block_mean = jnp.sum(turned, axis=0, keepdims=True) / 128
    block_m2 = jnp.sum(jnp.square(turned - block_mean), axis=0, keepdims=True)
    v.ss[0:1] = block_mean
    v.ss[1:2] = block_m2
    peers = [
        (k, core, 2 * k + j)
        for k in far_first + [0] for j, core in enumerate((c, oc)) if k or j
    ]
    for k, core, i in peers:
        send(v.ss, v.sr.at[i], "s", 0, zdev(k, core))
    whole(v.sr.at[pl.ds(0, ntp - 1)], "s").wait_recv()
    stats = [v.ss[...]] + [v.sr[i] for _, _, i in peers]
    mean = sum(s[0:1] for s in stats) / ntp
    m2 = sum(s[1:2] + 128 * jnp.square(s[0:1] - mean) for s in stats)
    scaled = ((turned - mean) * lax.rsqrt(m2 / d + NORM_EPS)).T
    v.out[...] = (scaled * v.second_gain[...]).astype(BF16)
    stores.append(pltpu.make_async_copy(v.out, lo_o, sem["store"].at[2]))
    stores[-1].start()
    for name, ref in (
        ("pm", v.pm_s), ("z", v.zs.at[pl.ds(0, nz - 1)]), ("st", v.st_s),
        ("ag", nrm.at[0, c, pl.ds(0, nz - 1)]), ("np", nrm.at[:, c]), ("nz", nrm.at[0, c]),
        ("dx", ds.at[pl.ds(0, ne - 1)]), ("xz", xin.at[0, c, pl.ds(0, len(beside) * nx)]),
        ("d2", xin.at[0, c, pl.ds(0, len(direct) * nx - 1)]), ("xp", xin.at[:, c]),
        ("po", v.ps), ("bz", v.bs), ("rt", v.rs.at[pl.ds(0, ne - 1)]), ("dp", v.dps),
        ("db", v.dbs), ("f", v.fs.at[pl.ds(0, hz - 1)]), ("s", v.sr.at[pl.ds(0, ntp - 1)]),
    ):
        if 0 not in ref.shape:
            whole(ref, name).wait_send()
    for copy in stores:
        copy.wait()


def hand_out(*refs):
    arrays, sem = refs[:9], refs[9]
    moves = [
        [pltpu.make_async_copy(arrays[i], arrays[6 + i], sem.at[i]) for i in range(3)],
        [pltpu.make_async_copy(arrays[6 + i], arrays[3 + i], sem.at[3 + i]) for i in range(3)],
    ]
    for copy in moves[0]:
        copy.start()
    for into, out in zip(*moves):
        into.wait()
        out.start()
    for copy in moves[1]:
        copy.wait()


def on_device(nz, ny, nx, *arrays):
    args = Args(*arrays)
    rows, d = args.tokens.shape
    ff = args.expert_gate.shape[2]
    args = args._replace(
        conv_state=args.conv_state.transpose(1, 0, 2),
        decay_param=args.decay_param.reshape(1, -1),
        first_gain=args.first_gain.reshape(1, -1),
        second_gain=args.second_gain.reshape(1, -1),
        expert_gate=args.expert_gate[0].T,
        expert_up=args.expert_up[0].T,
        expert_down=args.expert_down[0],
        routing=args.routing.T,
        route_weight=args.route_weight.T,
        mix_weight=args.mix_weight.reshape(-1, 128),
    )

    half, quarter = d // 2, d // 4
    ne, ntp, hz = ny * nx, 2 * nz, nz // 2
    cap = max(2, 2 * rows * TOPK // ne)
    group, zrow = nx * cap, rows // nz
    rows_at_once = min(2, ny) * group
    ng = ne * cap // rows_at_once
    scratch = {name: (a.shape, a.dtype) for name, a in args._asdict().items()}
    scratch.update(
        out_proj=((2, rows, half), BF16),
        expert_gate=((2, 2, ff, quarter), BF16), expert_up=((2, 2, ff, quarter), BF16),
        expert_down=((2, 2, ff, quarter), BF16),
        dense_gate=((2, 2, quarter, 128), BF16), dense_up=((2, 2, quarter, 128), BF16),
        dense_down=((2, 2, 128, quarter), BF16),
        pm_s=((rows, half), BF16), pm_r=((rows, half), BF16), pm_own=((rows, half), F32),
        state=((rows, 128), F32), window=((3, rows, 128), BF16), out=((rows, 128), BF16),
        zs=((nz, zrow, half), BF16), zr=((nz, zrow, half), BF16),
        st_s=((2, zrow, 128), F32), st_r=((2, zrow, 128), F32),
        nrm=((2, 2, nz, zrow, quarter), BF16), nother=((zrow, quarter), BF16),
        onehot=((ny, group, rows), BF16), wts=((2 * rows, ne * cap), BF16),
        ds=((ne, cap, quarter), BF16), ds2=((ne, cap, quarter), BF16),
        hidden=((ng, rows_at_once, ff), BF16), xin=((2, 2, ne, cap, quarter), BF16),
        ps=((ny, 2, group, quarter), BF16), pr=((ny, 2, group, quarter), BF16),
        po=((ny, 2, group, quarter), F32), gate=((ng, rows_at_once, ff), F32),
        up=((ng, rows_at_once, ff), F32),
        bs=((ny, group, quarter), BF16), br=((ny, group, quarter), BF16),
        rs=((ne, cap, quarter), BF16), ret=((ne, cap, quarter), BF16),
        mixf=((d // 128, 128), F32), mix=((rows, 128), F32),
        dps=((2, rows, quarter), BF16), dpr=((2, rows, quarter), BF16),
        dpo=((2, rows, quarter), F32), dbs=((rows, quarter), BF16), dbr=((rows, quarter), BF16),
        dacc=((rows, quarter), F32),
        fs=((hz, rows, 128), BF16), fr=((hz, rows, 128), BF16),
        ss=((2, rows), F32), sr=((ntp, 2, rows), F32),
    )
    pairs = dict(
        pm=1, z=1, st=1, ag=1, np=1, nz=1, dx=ny, d2=1, xz=ny, xp=2 * ny, po=2 * ny, bz=ny, rt=1, dp=1,
        db=1, f=1, s=1,
    )
    sems = {"load": len(args), "store": 3}
    for name, n in pairs.items():
        sems[name + "_s"], sems[name + "_r"] = 1, n
    anywhere = pl.BlockSpec(memory_space=pl.ANY)
    outs = (
        jax.ShapeDtypeStruct((rows, 128), BF16),
        jax.ShapeDtypeStruct((rows, 128), F32),
        jax.ShapeDtypeStruct((3, rows, 128), BF16),
    )
    labels = tuple(scratch), tuple(sems)
    results = pl.pallas_call(
        functools.partial(kernel, nz, ny, nx, cap, labels),
        name="decode_step",
        out_shape=outs,
        in_specs=[anywhere] * len(args),
        out_specs=(anywhere,) * 3,
        scratch_shapes=[pltpu.VMEM(*s) for s in scratch.values()]
        + [pltpu.SemaphoreType.DMA((n,)) for n in sems.values()],
        compiler_params=pltpu.CompilerParams(collective_id=0, has_side_effects=True),
    )(*args)
    layer_out, new_state, new_conv = pl.pallas_call(
        hand_out,
        name="hand_out",
        out_shape=outs,
        in_specs=[anywhere] * 3,
        out_specs=(anywhere,) * 3,
        scratch_shapes=[pltpu.VMEM(s.shape, s.dtype) for s in outs]
        + [pltpu.SemaphoreType.DMA((6,))],
    )(*results)
    return layer_out, new_state, new_conv.transpose(1, 0, 2)


def solution(mesh):
    ep, tp = mesh.shape["ep"], mesh.shape["tp"]
    nx = {16: 4, 4: 2, 2: 2}[ep]
    return jax.shard_map(
        functools.partial(on_device, tp // 2, ep // nx, nx),
        mesh=mesh,
        in_specs=(
            P("ep", None), P("ep", None, "tp"), P("ep", "tp"), P(None, "tp"), P(None, "tp"),
            P(None, "tp"), P("tp", None, None), P("tp", None, None), P("tp"), P("tp", None), P(),
            P("ep", None, "tp"), P("ep", None, "tp"), P("ep", "tp", None), P("ep", None),
            P("ep", None), P(None, "tp"), P(None, "tp"), P("tp", None), P(), P("tp"),
        ),
        out_specs=(P("ep", "tp"), P("ep", "tp"), P("ep", None, "tp")),
        check_vma=False,
    )
```

```python
import functools
from types import SimpleNamespace
from typing import Any, NamedTuple

import jax
import jax.numpy as jnp
from jax import lax
from jax.experimental import pallas as pl
from jax.experimental.pallas import tpu as pltpu
from jax.sharding import PartitionSpec as P

MESH = pl.DeviceIdType.MESH
ALPHA = 8.0**0.25
RATE_SCALE = 8.0
NORM_EPS = 1e-05
TOPK = 2
F32 = jnp.float32
BF16 = jnp.bfloat16


class Args(NamedTuple):
    tokens: Any
    conv_state: Any
    rec_state: Any
    gate_proj: Any
    input_proj: Any
    conv_taps: Any
    decay_blocks: Any
    input_blocks: Any
    decay_param: Any
    out_proj: Any
    first_gain: Any
    expert_gate: Any
    expert_up: Any
    expert_down: Any
    routing: Any
    route_weight: Any
    dense_gate: Any
    dense_up: Any
    dense_down: Any
    mix_weight: Any
    second_gain: Any


def dot(a, b):
    return jnp.dot(a, b, preferred_element_type=F32)


def dot_nt(a, b):
    return lax.dot_general(a, b, (((1,), (1,)), ((), ())), preferred_element_type=F32)


def one_less_exp(u):
    series = 1.0 - u * (1.0 / 8.0)
    for k in (7, 6, 5, 4, 3, 2):
        series = 1.0 - u * (1.0 / k) * series
    return jnp.where(u < 0.5, u * series, 1.0 - jnp.exp(-u))


def kernel(nz, ny, nx, cap, names, *refs):
    hbm = Args(*refs[: len(Args._fields)])
    refs = refs[len(hbm) :]
    lo_o, ns_o, nc_o = refs[:3]
    v = SimpleNamespace(**dict(zip(names[0], refs[3:])))
    sem = dict(zip(names[1], refs[3 + len(names[0]) :]))

    tok = v.tokens
    ne, ntp = ny * nx, 2 * nz
    rows, d = tok.shape
    half, quarter = d // 2, d // 4
    zrow, hz, group = rows // nz, nz // 2, nx * cap
    ep, tp = lax.axis_index("ep"), lax.axis_index("tp")
    z, c = lax.div(tp, 2), lax.rem(tp, 2)
    oc, q = 1 - c, lax.rem(z, 2)
    y, x = lax.div(ep, nx), lax.rem(ep, nx)
    partner = {"ep": ep, "tp": 2 * z + oc}

    def zdev(k, core):
        return {"ep": ep, "tp": 2 * lax.rem(z + k + nz, nz) + core}

    def edev(dy, dx):
        return lax.rem(y + dy + ny, ny) * nx + lax.rem(x + dx + nx, nx)

    def send(src, dst, name, i, dev):
        copy = pltpu.make_async_remote_copy(
            src_ref=src, dst_ref=dst,
            send_sem=sem[name + "_s"].at[0], recv_sem=sem[name + "_r"].at[i],
            device_id=dev, device_id_type=MESH,
        )
        copy.start()
        return copy

    def whole(ref, name, i=0):
        return pltpu.make_async_remote_copy(
            src_ref=ref, dst_ref=ref,
            send_sem=sem[name + "_s"].at[0], recv_sem=sem[name + "_r"].at[i],
            device_id=partner, device_id_type=MESH,
        )

    loads = {}

    def load(dst, *pieces):
        at = sem["load"].at[len(loads)]
        loads[id(dst)] = pltpu.make_async_copy(dst, dst, at)
        for src, part in pieces:
            pltpu.make_async_copy(src, part, at).start()

    def arrived(*wanted):
        for dst in wanted:
            loads[id(dst)].wait()

    for dst, src in (
        (v.tokens, hbm.tokens), (v.input_proj, hbm.input_proj), (v.gate_proj, hbm.gate_proj),
    ):
        load(dst, (src, dst))

    far_first = sorted(range(1, nz), key=lambda k: -min(k, nz - k))

    barrier = pltpu.get_barrier_semaphore()
    greeted = 0
    for k in far_first + [0]:
        for j, core in enumerate((c, oc)):
            if k or j:
                pl.semaphore_signal(barrier, inc=1, device_id=zdev(k, core), device_id_type=MESH)
                greeted += 1
    for dy in range(ny):
        for dx in range(nx):
            if dy or dx:
                pl.semaphore_signal(
                    barrier, inc=1, device_id={"ep": edev(dy, dx), "tp": tp}, device_id_type=MESH
                )
                greeted += 1

    for dst, src in (
        (v.conv_taps, hbm.conv_taps), (v.conv_state, hbm.conv_state),
        (v.decay_blocks, hbm.decay_blocks), (v.input_blocks, hbm.input_blocks),
        (v.decay_param, hbm.decay_param), (v.rec_state, hbm.rec_state),
    ):
        load(dst, (src, dst))
    load(v.out_proj, *[
        (hbm.out_proj.at[:, pl.ds(half * j, half)], v.out_proj.at[j]) for j in range(2)
    ])
    for dst, src in (
        (v.routing, hbm.routing), (v.route_weight, hbm.route_weight),
        (v.first_gain, hbm.first_gain),
    ):
        load(dst, (src, dst))
    starts = [
        (rel, core, pl.multiple_of(core * half + lax.rem(q + rel, 2) * quarter, quarter))
        for rel in range(2) for core in range(2)
    ]
    for dst, src in (v.dense_gate, hbm.dense_gate), (v.dense_up, hbm.dense_up):
        load(dst, *[
            (src.at[pl.ds(at, quarter), :], dst.at[rel, core]) for rel, core, at in starts
        ])
    for dst, src in (v.expert_gate, hbm.expert_gate), (v.expert_up, hbm.expert_up):
        load(dst, *[
            (src.at[:, pl.ds(at, quarter)], dst.at[rel, core]) for rel, core, at in starts
        ])
    for dst, src in (v.dense_down, hbm.dense_down), (v.expert_down, hbm.expert_down):
        load(dst, *[
            (
                src.at[:, pl.ds(128 * j, 128)],
                dst.at[j % 2, (j // 2) % 2, :, pl.ds(128 * (j // 4), 128)],
            )
            for j in range(ntp)
        ])
    for dst, src in (v.mix_weight, hbm.mix_weight), (v.second_gain, hbm.second_gain):
        load(dst, (src, dst))

    arrived(v.tokens, v.input_proj)
    inputs = dot(tok[...], v.input_proj[...]).astype(BF16)
    arrived(v.gate_proj)
    gated = dot(tok[...], v.gate_proj[...]).astype(BF16)
    arrived(v.conv_taps, v.conv_state, v.decay_blocks, v.input_blocks, v.decay_param, v.rec_state)
    taps = v.conv_taps[...].astype(F32)
    conv = inputs.astype(F32) * taps[3:4, :]
    for k in range(3):
        conv += v.conv_state[k].astype(F32) * taps[k : k + 1, :]
    convolved = conv.astype(BF16)
    recur_gate = jax.nn.sigmoid(dot(convolved, v.decay_blocks[0]))
    input_gate = jax.nn.sigmoid(dot(convolved, v.input_blocks[0]))
    param = v.decay_param[...]
    soft = jnp.maximum(-param, 0.0) + jnp.log1p(jnp.exp(-jnp.abs(param)))
    log_decay = -RATE_SCALE * recur_gate * soft
    state = jnp.exp(log_decay) * v.rec_state[...] + jnp.sqrt(
        one_less_exp(-2.0 * log_decay)
    ) * input_gate * convolved.astype(F32)
    g = gated.astype(F32)
    gelu = 0.5 * g * (1.0 + jnp.tanh(0.7978845608028654 * (g + 0.044715 * g * g * g)))
    mixed_rows = (state * gelu).astype(BF16)
    arrived(v.out_proj)
    v.pm_s[...] = dot(mixed_rows, v.out_proj[oc]).astype(BF16).reshape(nz, zrow, half)

    pl.semaphore_wait(barrier, greeted)

    pieces = [(i, k, lax.rem(z + k, nz)) for i, k in enumerate(far_first + [0])]
    swaps = [send(v.pm_s.at[at], v.pm_r.at[at], "pm", i, partner) for i, _, at in pieces]
    v.pm_own[...] = dot(mixed_rows, v.out_proj[c]).reshape(nz, zrow, half)
    v.state[...] = state
    v.window[0] = v.conv_state[1]
    v.window[1] = v.conv_state[2]
    v.window[2] = inputs
    stores = [
        pltpu.make_async_copy(v.state, ns_o, sem["store"].at[0]),
        pltpu.make_async_copy(v.window, nc_o, sem["store"].at[1]),
    ]
    for copy in stores:
        copy.start()
    for i, k, at in pieces:
        swaps[i].wait_recv()
        v.zs[at] = (v.pm_own[at] + v.pm_r[at].astype(F32)).astype(BF16)
        if k:
            send(v.zs.at[at], v.zr.at[z], "z", 0, zdev(k, c))

    arrived(v.routing, v.route_weight, v.first_gain)
    routes, route_weight = v.routing[...], v.route_weight[...]
    eids = lax.broadcasted_iota(jnp.int32, (ne, rows), 0)
    named = [routes[k : k + 1, :] == eids for k in range(TOPK)]
    either = jnp.where(named[0] | named[1], 1.0, 0.0)
    before = jnp.where(
        lax.broadcasted_iota(jnp.int32, (rows, rows), 0)
        < lax.broadcasted_iota(jnp.int32, (rows, rows), 1), 1.0, 0.0,
    )
    place = dot(either.astype(BF16), before.astype(BF16))
    slots = lax.broadcasted_iota(jnp.int32, (ne, cap, rows), 1).astype(F32)
    hit = (place[:, None, :] == slots) & (either[:, None, :] > 0.5)
    hot = jnp.where(hit, 1.0, 0.0)
    v.onehot[...] = hot.reshape(ny, group, rows).astype(BF16)
    weight = jnp.where(named[0], route_weight[0:1, :], 0.0)
    weight += jnp.where(named[1], route_weight[1:2, :], 0.0)
    weighted = (hot * weight[:, None, :]).reshape(ne * cap, rows).T
    upper = weighted.astype(BF16)
    v.wts[0:rows, :] = upper
    v.wts[rows:, :] = (weighted - upper.astype(F32)).astype(BF16)

    my_rows = pl.ds(pl.multiple_of(z * zrow, zrow), zrow)
    my_cols = pl.ds(pl.multiple_of(c * half, half), half)
    total = ALPHA * tok[my_rows, my_cols].astype(F32) + v.zs[z].astype(F32)
    whole(v.zr.at[pl.ds(0, nz - 1)], "z").wait_recv()
    for k in range(1, nz):
        total += v.zr[lax.rem(z - k + nz, nz)].astype(F32)

    row_mean = jnp.sum(total, axis=1, keepdims=True) / half
    row_m2 = jnp.sum(jnp.square(total - row_mean), axis=1, keepdims=True)
    v.st_s[0] = jnp.broadcast_to(row_mean, (zrow, 128))
    v.st_s[1] = jnp.broadcast_to(row_m2, (zrow, 128))
    send(v.st_s, v.st_r, "st", 0, partner).wait_recv()
    peer_mean, peer_m2 = v.st_r[0][:, 0:1], v.st_r[1][:, 0:1]
    mean = 0.5 * (row_mean + peer_mean)
    variance = (row_m2 + peer_m2 + jnp.square(row_mean - peer_mean) * (half / 2)) / d
    normed = (
        (total - mean) * lax.rsqrt(variance + NORM_EPS) * v.first_gain[:, my_cols]
    ).astype(BF16)
    first, second = normed[:, 0:quarter], normed[:, quarter:]
    even = q == 0
    nrm = v.nrm
    v.nother[...] = jnp.where(even, second, first)
    nrm[0, c, z] = jnp.where(even, first, second)

    for k in far_first:
        send(v.nother if k % 2 else nrm.at[0, c, z], nrm.at[0, c, z], "ag", 0, zdev(k, c))
    whole(nrm.at[0, c, pl.ds(0, nz - 1)], "ag").wait_recv()

    xin, ds = v.xin, v.ds
    offsets = [(dy, dx) for dy in range(ny) for dx in range(nx)]
    if ny == nx == 4:
        offsets = [
            (2, 2), (3, 2), (2, 3), (2, 1), (1, 2), (3, 1), (1, 3), (2, 0),
            (0, 2), (3, 3), (1, 1), (3, 0), (1, 0), (0, 3), (0, 1), (0, 0),
        ]
    direct = {ny - 1}
    beside = [f for f in range(ny) if f not in direct]

    def members(f):
        return list(enumerate(offsets))[f * nx : (f + 1) * nx]

    def dispatch(f, rel, out, name, at, done):
        for p, (dy, dx) in members(f):
            yy, e = lax.rem(y + dy, ny), edev(dy, dx)
            if dy not in done:
                done.add(dy)
                out[pl.ds(yy * nx, nx)] = dot(
                    v.onehot[yy], nrm[rel, c].reshape(rows, quarter)
                ).astype(BF16).reshape(nx, cap, quarter)
        for p, (dy, dx) in members(f):
            if dy or dx:
                e = edev(dy, dx)
                send(out.at[e], xin.at[rel, c, p], name, at, {"ep": e, "tp": tp})
            else:
                xin[rel, c, p] = out[ep]

    done = set()
    for f in range(ny):
        dispatch(f, 0, ds, "dx", f, done)

    first_z, last_z = pl.ds(0, hz), pl.ds(hz, hz)
    for part, k in (first_z, 1), (last_z, -1):
        send(nrm.at[0, c, part], nrm.at[1, c, part], "nz", 0, zdev(k, c))
    send(nrm.at[0, c], nrm.at[0, c], "np", 0, partner)

    per = min(2, ny)
    flight = {}

    def halves(src, dst, count, name, at):
        for part, k in (pl.ds(0, count // 2), 1), (pl.ds(count // 2, count // 2), -1):
            send(src.at[part], dst.at[part], name, at, zdev(k, c))
        return whole(dst, name, at)

    def normed_beside(_):
        whole(nrm.at[1, c], "nz").wait_recv()
        send(nrm.at[1, c], nrm.at[1, c], "np", 0, partner)
        done = set()
        for f in sorted(direct):
            dispatch(f, 1, v.ds2, "d2", 0, done)

    def arrive(f):
        count = len([p for p, at in members(f) if at != (0, 0)])
        whole(xin.at[0, c, pl.ds(f * nx, count)], "dx", f).wait_recv()
        row = pl.ds(f * nx, nx)
        if f not in direct:
            flight["z", f] = halves(xin.at[0, c, row], xin.at[1, c, row], nx, "xz", f)
        flight["own", f] = send(xin.at[0, c, row], xin.at[0, c, row], "xp", 2 * f, partner)

    def hand_over(f):
        if f not in direct:
            flight["z", f].wait_recv()
        else:
            count = len([p for p, at in members(f) if at != (0, 0)])
            whole(xin.at[1, c, pl.ds(f * nx, count)], "d2").wait_recv()
        row = pl.ds(f * nx, nx)
        flight["other", f] = send(xin.at[1, c, row], xin.at[1, c, row], "xp", 2 * f + 1, partner)

    def gate_up(k, rel):
        pieces = [
            xin[rel, core, pl.ds(k * per * nx, per * nx)].reshape(per * group, quarter)
            for core in range(2)
        ]
        return [
            dot_nt(pieces[0], weights[rel, 0]) + dot_nt(pieces[1], weights[rel, 1])
            for weights in (v.expert_gate, v.expert_up)
        ]

    def compute_own(k):
        if k == 0:
            arrived(v.expert_gate, v.expert_up)
        for f in range(k * per, (k + 1) * per):
            flight["own", f].wait_recv()
        v.gate[k], v.up[k] = gate_up(k, 0)

    def compute_other(k):
        for f in range(k * per, (k + 1) * per):
            flight["other", f].wait_recv()
        gate, up = gate_up(k, 1)
        v.hidden[k] = (jax.nn.silu(v.gate[k] + gate) * (v.up[k] + up)).astype(BF16)

    def down(k):
        fine = range(k * per, (k + 1) * per)
        if k == 0:
            arrived(v.expert_down)
        hidden = v.hidden[k]
        for j, par in enumerate((1 - q, q)):
            product = dot(hidden, v.expert_down[oc, par]).astype(BF16)
            for f in fine:
                at = (f - k * per) * group
                v.ps[f, j] = product[at : at + group]
                flight["sum", f, j] = send(
                    v.ps.at[f, j], v.pr.at[f, j], "po", 2 * f + j, partner
                )
        for j, par in enumerate((1 - q, q)):
            product = dot(hidden, v.expert_down[c, par])
            for f in fine:
                at = (f - k * per) * group
                v.po[f, j] = product[at : at + group]

    def pair_sum(f):
        flight["sum", f, 0].wait_recv()
        v.bs[f] = (v.po[f, 0] + v.pr[f, 0].astype(F32)).astype(BF16)
        flight["beside", f] = halves(v.bs.at[f], v.br.at[f], group, "bz", f)

    def go_home(f):
        flight["sum", f, 1].wait_recv()
        flight["beside", f].wait_recv()
        v.rs[pl.ds(f * nx, nx)] = (
            v.po[f, 1] + v.pr[f, 1].astype(F32) + v.br[f].astype(F32)
        ).astype(BF16).reshape(nx, cap, quarter)
        for p, (dy, dx) in members(f):
            if dy or dx:
                home = {"ep": edev(-dy, -dx), "tp": tp}
                send(v.rs.at[p], v.ret.at[ep], "rt", 0, home)
            else:
                v.ret[ep] = v.rs[p]

    def dense_start(_):
        arrived(v.dense_gate, v.dense_up, v.dense_down, v.mix_weight)
        whole(nrm.at[:, c], "np").wait_recv()
        gate = up = mixing = None
        v.mixf[...] = v.mix_weight[...].astype(F32)
        for rel, core, _ in starts:
            piece = nrm[rel, core].reshape(rows, quarter)
            more = dot(piece, v.dense_gate[rel, core])
            gate = more if gate is None else gate + more
            more = dot(piece, v.dense_up[rel, core])
            up = more if up is None else up + more
            for j in range(quarter // 128):
                at = (core * 2 + lax.rem(q + rel, 2)) * (quarter // 128) + j
                more = piece[:, 128 * j : 128 * (j + 1)].astype(F32) * v.mixf[pl.ds(at, 1), :]
                mixing = more if mixing is None else mixing + more
        hidden = (jax.nn.silu(gate) * up).astype(BF16)
        for j, par in enumerate((1 - q, q)):
            v.dps[j] = dot(hidden, v.dense_down[oc, par]).astype(BF16)
        flight["dense"] = send(v.dps, v.dpr, "dp", 0, partner)
        for j, par in enumerate((1 - q, q)):
            v.dpo[j] = dot(hidden, v.dense_down[c, par])
        v.mix[...] = jnp.broadcast_to(
            jax.nn.sigmoid(jnp.sum(mixing, axis=1, keepdims=True)), (rows, 128)
        )

    def dense_pair(_):
        flight["dense"].wait_recv()
        v.dbs[...] = (v.dpo[0] + v.dpr[0].astype(F32)).astype(BF16)
        flight["dense_beside"] = halves(v.dbs, v.dbr, rows, "db", 0)

    def dense_end(_):
        flight["dense_beside"].wait_recv()
        v.dacc[...] = v.mix[:, 0:1] * (
            v.dpo[1] + v.dpr[1].astype(F32) + v.dbr[...].astype(F32)
        )

    plan = [
        (normed_beside, 0), (arrive, 0), (arrive, 1), (arrive, 2), (dense_start, 0), (arrive, 3),
        (hand_over, 0), (compute_own, 0), (hand_over, 1), (hand_over, 3), (compute_own, 1),
        (compute_other, 0), (hand_over, 2), (down, 0), (pair_sum, 0), (pair_sum, 1),
        (compute_other, 1), (down, 1), (pair_sum, 2), (pair_sum, 3), (dense_pair, 0), (go_home, 0),
        (go_home, 1), (go_home, 2), (go_home, 3), (dense_end, 0),
    ]
    for step, which in plan:
        if which < (ny // per if step in (compute_own, compute_other, down) else ny):
            step(which)

    whole(v.ret.at[pl.ds(0, ne - 1)], "rt").wait_recv()
    both = dot(v.wts[...], v.ret[...].reshape(ne * cap, quarter))
    fin = v.dacc[...] + both[0:rows] + both[rows:]
    for k in range(hz):
        v.fs[k] = fin[:, 128 * k : 128 * (k + 1)].astype(BF16)
    zh = lax.div(z, 2)
    for k in sorted(range(1, hz), key=lambda k: -min(k, hz - k)):
        send(v.fs.at[lax.rem(zh + k, hz)], v.fr.at[zh], "f", 0, zdev(2 * k, c))
    place_of = lax.rem(tp, nz)
    column = pl.ds(pl.multiple_of(lax.rem(place_of, hz) * 128, 128), 128)
    own = nrm[lax.rem(lax.div(place_of, hz) + q, 2), lax.div(tp, nz), :, :, column]
    combined = ALPHA * own.reshape(rows, 128).astype(F32) + v.fs[zh].astype(F32)
    if hz > 1:
        whole(v.fr.at[pl.ds(0, hz - 1)], "f").wait_recv()
    for k in range(1, hz):
        combined += v.fr[lax.rem(zh - k + hz, hz)].astype(F32)

    arrived(v.second_gain)
    turned = combined.T
    block_mean = jnp.sum(turned, axis=0, keepdims=True) / 128
    block_m2 = jnp.sum(jnp.square(turned - block_mean), axis=0, keepdims=True)
    v.ss[0:1] = block_mean
    v.ss[1:2] = block_m2
    peers = [
        (k, core, 2 * k + j)
        for k in far_first + [0] for j, core in enumerate((c, oc)) if k or j
    ]
    for k, core, i in peers:
        send(v.ss, v.sr.at[i], "s", 0, zdev(k, core))
    whole(v.sr.at[pl.ds(0, ntp - 1)], "s").wait_recv()
    stats = [v.ss[...]] + [v.sr[i] for _, _, i in peers]
    mean = sum(s[0:1] for s in stats) / ntp
    m2 = sum(s[1:2] + 128 * jnp.square(s[0:1] - mean) for s in stats)
    scaled = ((turned - mean) * lax.rsqrt(m2 / d + NORM_EPS)).T
    v.out[...] = (scaled * v.second_gain[...]).astype(BF16)
    stores.append(pltpu.make_async_copy(v.out, lo_o, sem["store"].at[2]))
    stores[-1].start()
    for name, ref in (
        ("pm", v.pm_s), ("z", v.zs.at[pl.ds(0, nz - 1)]), ("st", v.st_s),
        ("ag", nrm.at[0, c, pl.ds(0, nz - 1)]), ("np", nrm.at[:, c]), ("nz", nrm.at[0, c]),
        ("dx", ds.at[pl.ds(0, ne - 1)]), ("xz", xin.at[0, c, pl.ds(0, len(beside) * nx)]),
        ("d2", xin.at[0, c, pl.ds(0, len(direct) * nx - 1)]), ("xp", xin.at[:, c]),
        ("po", v.ps), ("bz", v.bs), ("rt", v.rs.at[pl.ds(0, ne - 1)]), ("dp", v.dps),
        ("db", v.dbs), ("f", v.fs.at[pl.ds(0, hz - 1)]), ("s", v.sr.at[pl.ds(0, ntp - 1)]),
    ):
        if 0 not in ref.shape:
            whole(ref, name).wait_send()
    for copy in stores:
        copy.wait()


def hand_out(*refs):
    arrays, sem = refs[:9], refs[9]
    moves = [
        [pltpu.make_async_copy(arrays[i], arrays[6 + i], sem.at[i]) for i in range(3)],
        [pltpu.make_async_copy(arrays[6 + i], arrays[3 + i], sem.at[3 + i]) for i in range(3)],
    ]
    for copy in moves[0]:
        copy.start()
    for into, out in zip(*moves):
        into.wait()
        out.start()
    for copy in moves[1]:
        copy.wait()


def on_device(nz, ny, nx, *arrays):
    args = Args(*arrays)
    rows, d = args.tokens.shape
    ff = args.expert_gate.shape[2]
    args = args._replace(
        conv_state=args.conv_state.transpose(1, 0, 2),
        decay_param=args.decay_param.reshape(1, -1),
        first_gain=args.first_gain.reshape(1, -1),
        second_gain=args.second_gain.reshape(1, -1),
        expert_gate=args.expert_gate[0].T,
        expert_up=args.expert_up[0].T,
        expert_down=args.expert_down[0],
        routing=args.routing.T,
        route_weight=args.route_weight.T,
        mix_weight=args.mix_weight.reshape(-1, 128),
    )

    half, quarter = d // 2, d // 4
    ne, ntp, hz = ny * nx, 2 * nz, nz // 2
    cap = max(2, 2 * rows * TOPK // ne)
    group, zrow = nx * cap, rows // nz
    rows_at_once = min(2, ny) * group
    ng = ne * cap // rows_at_once
    scratch = {name: (a.shape, a.dtype) for name, a in args._asdict().items()}
    scratch.update(
        out_proj=((2, rows, half), BF16),
        expert_gate=((2, 2, ff, quarter), BF16), expert_up=((2, 2, ff, quarter), BF16),
        expert_down=((2, 2, ff, quarter), BF16),
        dense_gate=((2, 2, quarter, 128), BF16), dense_up=((2, 2, quarter, 128), BF16),
        dense_down=((2, 2, 128, quarter), BF16),
        pm_s=((nz, zrow, half), BF16), pm_r=((nz, zrow, half), BF16),
        pm_own=((nz, zrow, half), F32),
        state=((rows, 128), F32), window=((3, rows, 128), BF16), out=((rows, 128), BF16),
        zs=((nz, zrow, half), BF16), zr=((nz, zrow, half), BF16),
        st_s=((2, zrow, 128), F32), st_r=((2, zrow, 128), F32),
        nrm=((2, 2, nz, zrow, quarter), BF16), nother=((zrow, quarter), BF16),
        onehot=((ny, group, rows), BF16), wts=((2 * rows, ne * cap), BF16),
        ds=((ne, cap, quarter), BF16), ds2=((ne, cap, quarter), BF16),
        hidden=((ng, rows_at_once, ff), BF16), xin=((2, 2, ne, cap, quarter), BF16),
        ps=((ny, 2, group, quarter), BF16), pr=((ny, 2, group, quarter), BF16),
        po=((ny, 2, group, quarter), F32), gate=((ng, rows_at_once, ff), F32),
        up=((ng, rows_at_once, ff), F32),
        bs=((ny, group, quarter), BF16), br=((ny, group, quarter), BF16),
        rs=((ne, cap, quarter), BF16), ret=((ne, cap, quarter), BF16),
        mixf=((d // 128, 128), F32), mix=((rows, 128), F32),
        dps=((2, rows, quarter), BF16), dpr=((2, rows, quarter), BF16),
        dpo=((2, rows, quarter), F32), dbs=((rows, quarter), BF16), dbr=((rows, quarter), BF16),
        dacc=((rows, quarter), F32),
        fs=((hz, rows, 128), BF16), fr=((hz, rows, 128), BF16),
        ss=((2, rows), F32), sr=((ntp, 2, rows), F32),
    )
    pairs = dict(
        pm=nz, z=1, st=1, ag=1, np=1, nz=1, dx=ny, d2=1, xz=ny, xp=2 * ny, po=2 * ny, bz=ny, rt=1, dp=1,
        db=1, f=1, s=1,
    )
    sems = {"load": len(args), "store": 3}
    for name, n in pairs.items():
        sems[name + "_s"], sems[name + "_r"] = 1, n
    anywhere = pl.BlockSpec(memory_space=pl.ANY)
    outs = (
        jax.ShapeDtypeStruct((rows, 128), BF16),
        jax.ShapeDtypeStruct((rows, 128), F32),
        jax.ShapeDtypeStruct((3, rows, 128), BF16),
    )
    labels = tuple(scratch), tuple(sems)
    results = pl.pallas_call(
        functools.partial(kernel, nz, ny, nx, cap, labels),
        name="decode_step",
        out_shape=outs,
        in_specs=[anywhere] * len(args),
        out_specs=(anywhere,) * 3,
        scratch_shapes=[pltpu.VMEM(*s) for s in scratch.values()]
        + [pltpu.SemaphoreType.DMA((n,)) for n in sems.values()],
        compiler_params=pltpu.CompilerParams(collective_id=0, has_side_effects=True),
    )(*args)
    layer_out, new_state, new_conv = pl.pallas_call(
        hand_out,
        name="hand_out",
        out_shape=outs,
        in_specs=[anywhere] * 3,
        out_specs=(anywhere,) * 3,
        scratch_shapes=[pltpu.VMEM(s.shape, s.dtype) for s in outs]
        + [pltpu.SemaphoreType.DMA((6,))],
    )(*results)
    return layer_out, new_state, new_conv.transpose(1, 0, 2)


def solution(mesh):
    ep, tp = mesh.shape["ep"], mesh.shape["tp"]
    nx = {16: 4, 4: 2, 2: 2}[ep]
    return jax.shard_map(
        functools.partial(on_device, tp // 2, ep // nx, nx),
        mesh=mesh,
        in_specs=(
            P("ep", None), P("ep", None, "tp"), P("ep", "tp"), P(None, "tp"), P(None, "tp"),
            P(None, "tp"), P("tp", None, None), P("tp", None, None), P("tp"), P("tp", None), P(),
            P("ep", None, "tp"), P("ep", None, "tp"), P("ep", "tp", None), P("ep", None),
            P("ep", None), P(None, "tp"), P(None, "tp"), P("tp", None), P(), P("tp"),
        ),
        out_specs=(P("ep", "tp"), P("ep", "tp"), P("ep", None, "tp")),
        check_vma=False,
    )
```
